512 devices in a mesh: ep: 128 (over z, y, core), tp: 4 (over x).
Axes of the slice: x: 4, y: 8, z: 8, core: 2. Of those that a mesh axis runs over, the one named last changes fastest.
Arguments:
- tokens: bfloat16 [2304, 1024], P('ep'), may hold values from -16 to 16
- delta_state: float32 [2304, 4, 128, 128], P('ep', 'tp'), may hold values from -1.8 to 1.8
- mixer_gain: float32 [1024], replicated, may hold values from 0.1 to 1.9
- query_weight: bfloat16 [1024, 512], P(None, 'tp'), may hold values from -0.1875 to 0.1875
- key_weight: bfloat16 [1024, 512], P(None, 'tp'), may hold values from -0.1875 to 0.1875
- value_weight: bfloat16 [1024, 512], P(None, 'tp'), may hold values from -0.1875 to 0.1875
- write_weight: bfloat16 [1024, 4], P(None, 'tp'), may hold values from -0.1875 to 0.1875
- decay_weight: bfloat16 [1024, 4], P(None, 'tp'), may hold values from -0.1875 to 0.1875
- decay_rate: float32 [4], P('tp'), may hold values from 0.05 to 4
- decay_bias: float32 [4], P('tp'), may hold values from -2 to 1
- head_gain: float32 [128], replicated, may hold values from 0.1 to 1.9
- out_weight: bfloat16 [512, 1024], P('tp'), may hold values from -0.25 to 0.25
- channel_gain: float32 [1024], replicated, may hold values from 0.1 to 1.9
- routes: int32 [2304, 6], P('ep'), may hold values from 0 to 127, all different within a row; in each aligned block of 18 rows (0 to 17, 18 to 35, ...) at most 2 rows name the same one
- route_weights: float32 [2304, 6], P('ep'), may hold values from 0.1 to 1
- expert_gate: bfloat16 [128, 1024, 512], P('ep', None, 'tp'), may hold values from -0.1875 to 0.1875
- expert_up: bfloat16 [128, 1024, 512], P('ep', None, 'tp'), may hold values from -0.1875 to 0.1875
- expert_down: bfloat16 [128, 512, 1024], P('ep', 'tp'), may hold values from -0.25 to 0.25
- shared_gate: bfloat16 [1024, 512], P(None, 'tp'), may hold values from -0.1875 to 0.1875
- shared_up: bfloat16 [1024, 512], P(None, 'tp'), may hold values from -0.1875 to 0.1875
- shared_down: bfloat16 [512, 1024], P('tp'), may hold values from -0.25 to 0.25
Outputs:
- layer_out: bfloat16 [2304, 1024], P('ep', 'tp')
- next_state: float32 [2304, 4, 128, 128], P('ep', 'tp')
The draws below stay inside these ranges and needn't reach their ends.
Inputs may be any that keep to these rules, and one draw needn't show every extreme that they name: `routes`: each row names 6 different experts. In each aligned block of 18 rows (the rows of one ep index) no expert is named by more than 2 rows, a bound that some block reaches.
All inputs are finite; a program needn't handle non-finite values.
Results may differ from the reference program's by a relative error of at most 0.015.
Values may be sent and summed in bfloat16 or wider, within the bound.
No kernel may reach another device: no remote copies, remote signals or barrier semaphores. Data moves between devices by JAX's collectives and lax.ppermute only.
A program may use at most 64 MiB of HBM per device.

```python
import math
import jax
import jax.numpy as jnp
import numpy as np
from jax import lax

D = 1024
HEADS = 4
HEAD_DIM = 128
D_EXPERT = 512
D_SHARED = 512
EXPERTS = 128
TOP_K = 6
SEQ_DEV = 18
CAP = 2
TOKENS = 2304
N_EP = 128
N_TP = 4


def draw_tokens(key, part):
    entry_key, column_key = jax.random.split(jax.random.fold_in(key, 71))
    column_pos = jnp.arange(D, dtype=jnp.float32) / (D - 1)
    jitter = jnp.exp(jax.random.uniform(column_key, (D,), jnp.float32, jnp.log(0.7), jnp.log(1.4)))
    rise = jnp.exp(jnp.log(0.5) + column_pos * jnp.log(5.0))
    entries = jnp.clip(jax.random.normal(entry_key, (TOKENS, D), jnp.float32), -4.0, 4.0)
    return (entries * (rise * jitter)[None, :]).astype(jnp.bfloat16)


def levels(stream_key, extent, shards, low, top_value):
    loudness, own = 1.0, jax.random.fold_in(stream_key, 6)
    for position, shards_of in shards:
        heights = jnp.exp(jax.random.uniform(jax.random.fold_in(own, position), (shards_of,), jnp.float32, low / len(shards), top_value / len(shards)))
        loudness = loudness * jnp.repeat(heights, extent[position] // shards_of).reshape([-1 if axis == position else 1 for axis in range(len(extent))])
    return loudness


def deal_out(stream_key, own, number, rows, count, top, most, slope):
    ranking = jax.random.permutation(stream_key, count)
    heavy_load, common = shares(count, rows * top, most, slope, True), shares(count, rows * top, most, slope, False)
    places = jnp.arange(count)

    def named(tallies, rotation):
        used = int((tallies > 0).sum())
        fixed = max(1, used // 4)
        passed = fixed + (places - fixed + rotation * (used - fixed)) % max(1, count - fixed)
        return jnp.zeros((count,), jnp.int32).at[ranking[jnp.where(places < fixed, places, passed)]].set(jnp.asarray(tallies, jnp.int32))

    tallies = jnp.where(number % 4 == 0, named(heavy_load, number // 4), named(common, number - number // 4 - 1))
    mixed = jax.random.permutation(jax.random.fold_in(own, 3), count)
    source_of, sink = mixed[0:count // 2 * 2:2], mixed[1:count // 2 * 2:2]
    slack = jnp.minimum(tallies[source_of] - 1, most - tallies[sink]) // 2
    slack = jnp.where((source_of == ranking[0]) | (sink == ranking[0]) | (tallies[sink] == 0), 0, jnp.maximum(slack, 0))
    passed = jax.random.randint(jax.random.fold_in(own, 4), (count // 2,), 0, 1 << 20) % (slack + 1)
    tallies = tallies.at[source_of].add(-passed).at[sink].add(passed)
    members = jnp.searchsorted(jnp.cumsum(tallies), jnp.arange(rows * top), side="right").astype(jnp.int32)
    table = members.reshape(top, rows).T
    table = table[jax.random.permutation(jax.random.fold_in(own, 1), rows)]
    rotation = jax.random.randint(jax.random.fold_in(own, 2), (rows, 1), 0, top)
    return jnp.take_along_axis(table, (jnp.arange(top)[None, :] + rotation) % top, axis=1)


def shares(count, total, limit, skew, full):
    loads = [(1 << 20) // math.isqrt(rank ** skew) + 1 for rank in range(1, count + 1)]
    largest = limit if full else min(limit, max(-(-total // count), total * loads[0] // sum(loads)))
    least = 1 if total - largest >= count - 1 else 0
    counts, surplus = [largest] + [least] * (count - 1), total - largest - least * (count - 1)
    while surplus > 0:
        movable = [i for i in range(1, count) if counts[i] < largest] or [i for i in range(1, count) if counts[i] < limit]
        whole, budget = sum([loads[i] for i in movable]), surplus
        for i in movable:
            more = min(limit - counts[i], max(1, budget * loads[i] // whole), surplus)
            counts[i] = counts[i] + more
            surplus = surplus - more
    return np.array(counts)


def gaussian(own_key, shape, deviation, reach, shards=(), kind=jnp.bfloat16):
    drawn = jax.random.normal(own_key, shape, jnp.float32) * deviation
    if len(shards) > 0:
        drawn = levels(own_key, shape, shards, -0.22, 0.18) * drawn
    return jnp.clip(drawn, min=-reach, max=reach).astype(kind)


def setup_inputs(seed: int = 0) -> dict:
    seeds = jax.random.split(jax.random.key(seed), 22)
    tokens = draw_tokens(jax.random.fold_in(seeds[21], 71), 0)
    delta_state = gaussian(seeds[1], (TOKENS, HEADS, HEAD_DIM, HEAD_DIM), 0.3, 1.8, ((0, 128), (1, 4)), jnp.float32)
    mixer_gain = jnp.clip(1.0 + 0.18 * jax.random.normal(seeds[2], (D,), jnp.float32), 0.1, 1.9)
    query_weight = gaussian(seeds[3], (D, HEADS * HEAD_DIM), D ** -0.5, 0.1875, ((1, 4),))
    key_weight = gaussian(seeds[4], (D, HEADS * HEAD_DIM), D ** -0.5, 0.1875, ((1, 4),))
    value_weight = gaussian(seeds[5], (D, HEADS * HEAD_DIM), D ** -0.5, 0.1875, ((1, 4),))
    write_weight = gaussian(seeds[6], (D, HEADS), D ** -0.5, 0.1875, ((1, 4),))
    decay_weight = gaussian(seeds[7], (D, HEADS), D ** -0.5, 0.1875, ((1, 4),))
    decay_rate = jnp.clip(jnp.exp(math.log(4.0) - 4.3820266 * jax.random.uniform(seeds[8], (HEADS,), jnp.float32) ** levels(seeds[8], (HEADS,), ((0, 4),), -0.2, 0.2)), 0.05, 4.0)
    decay_bias = jnp.clip(-2.0 + 3.0 * jax.random.uniform(seeds[9], (HEADS,), jnp.float32) ** levels(seeds[9], (HEADS,), ((0, 4),), -0.2, 0.2), -2.0, 1.0)
    head_gain = jnp.clip(1.0 + 0.18 * jax.random.normal(seeds[10], (HEAD_DIM,), jnp.float32), 0.1, 1.9)
    out_weight = gaussian(seeds[11], (HEADS * HEAD_DIM, D), (HEADS * HEAD_DIM) ** -0.5, 0.25, ((0, 4),))
    channel_gain = jnp.clip(1.0 + 0.18 * jax.random.normal(seeds[12], (D,), jnp.float32), 0.1, 1.9)
    routes_keys = jax.random.split(jax.random.fold_in(seeds[13], 1), TOKENS // SEQ_DEV)
    routes_turns = jax.random.permutation(jax.random.fold_in(seeds[13], 3), TOKENS // SEQ_DEV)
    routes = jax.vmap(lambda own, number: deal_out(jax.random.fold_in(seeds[13], 2), own, number, SEQ_DEV, EXPERTS, TOP_K, CAP, 1))(routes_keys, routes_turns).reshape((TOKENS, TOP_K))
    route_weights = jnp.clip(jnp.exp(math.log(1.0) - 2.3025851 * jax.random.uniform(seeds[14], (TOKENS, TOP_K), jnp.float32) ** levels(seeds[14], (TOKENS, TOP_K), ((0, 128),), -0.2, 0.2)), 0.1, 1.0)
    expert_gate = gaussian(seeds[15], (EXPERTS, D, D_EXPERT), D ** -0.5, 0.1875, ((0, 128), (2, 4)))
    expert_up = gaussian(seeds[16], (EXPERTS, D, D_EXPERT), D ** -0.5, 0.1875, ((0, 128), (2, 4)))
    expert_down = gaussian(seeds[17], (EXPERTS, D_EXPERT, D), D_EXPERT ** -0.5, 0.25, ((0, 128), (1, 4)))
    shared_gate = gaussian(seeds[18], (D, D_SHARED), D ** -0.5, 0.1875, ((1, 4),))
    shared_up = gaussian(seeds[19], (D, D_SHARED), D ** -0.5, 0.1875, ((1, 4),))
    shared_down = gaussian(seeds[20], (D_SHARED, D), D_SHARED ** -0.5, 0.25, ((0, 4),))
    return dict(tokens=tokens, delta_state=delta_state, mixer_gain=mixer_gain, query_weight=query_weight, key_weight=key_weight, value_weight=value_weight, write_weight=write_weight, decay_weight=decay_weight, decay_rate=decay_rate, decay_bias=decay_bias, head_gain=head_gain, out_weight=out_weight, channel_gain=channel_gain, routes=routes, route_weights=route_weights, expert_gate=expert_gate, expert_up=expert_up, expert_down=expert_down, shared_gate=shared_gate, shared_up=shared_up, shared_down=shared_down)


EPS = 1e-06
ROUTED_SCALE = 2.5

def rms_rows(values, gain_vec):
    mean_square = lax.optimization_barrier(jnp.mean(values * values, axis=-1, keepdims=True))
    return values * lax.rsqrt(mean_square + EPS) * gain_vec.astype(jnp.float32)

def unit_heads(raw, heads, head_dim):
    shaped = raw.astype(jnp.float32).reshape(raw.shape[0], heads, head_dim)
    return shaped * lax.rsqrt(lax.optimization_barrier(jnp.sum(shaped * shaped, axis=-1, keepdims=True)) + EPS)

def group_sum(hidden, weight, groups):
    group_width = hidden.shape[1] // groups
    running = jnp.zeros((hidden.shape[0], weight.shape[1]), jnp.float32)
    for group_number in range(groups):
        lower = group_number * group_width
        product = jnp.dot(hidden[:, lower:lower + group_width], weight[lower:lower + group_width], preferred_element_type=jnp.float32)
        rounded = lax.optimization_barrier(product.astype(jnp.bfloat16))
        running = running + rounded.astype(jnp.float32)
    return running.astype(jnp.bfloat16)

def reference(tokens, delta_state, mixer_gain, query_weight, key_weight, value_weight, write_weight, decay_weight, decay_rate, decay_bias, head_gain, out_weight, channel_gain, routes, route_weights, expert_gate, expert_up, expert_down, shared_gate, shared_up, shared_down):
    rows_total = tokens.shape[0]
    normed = rms_rows(tokens.astype(jnp.float32), mixer_gain).astype(jnp.bfloat16)
    query_raw = jnp.dot(normed, query_weight, preferred_element_type=jnp.float32).astype(jnp.bfloat16)
    key_raw = jnp.dot(normed, key_weight, preferred_element_type=jnp.float32).astype(jnp.bfloat16)
    value_raw = jnp.dot(normed, value_weight, preferred_element_type=jnp.float32).astype(jnp.bfloat16)
    write_rate = jax.nn.sigmoid(jnp.dot(normed, write_weight, preferred_element_type=jnp.float32))
    decay_keep = jnp.exp(-decay_rate * jax.nn.softplus(jnp.dot(normed, decay_weight, preferred_element_type=jnp.float32) + decay_bias))
    query_unit = unit_heads(query_raw, HEADS, HEAD_DIM) * HEAD_DIM ** (-0.5)
    key_unit = unit_heads(key_raw, HEADS, HEAD_DIM)
    value_vec = value_raw.astype(jnp.float32).reshape(rows_total, HEADS, HEAD_DIM)
    held_state = decay_keep[:, :, None, None] * delta_state
    correction = value_vec - jnp.einsum('rhkv,rhk->rhv', held_state, key_unit, precision=lax.Precision.HIGHEST)
    next_state = held_state + write_rate[:, :, None, None] * key_unit[:, :, :, None] * correction[:, :, None, :]
    readout = jnp.einsum('rhkv,rhk->rhv', next_state, query_unit, precision=lax.Precision.HIGHEST)
    head_out = rms_rows(readout, head_gain).astype(jnp.bfloat16).reshape(rows_total, HEADS * HEAD_DIM)
    mixer_out = group_sum(head_out, out_weight, N_TP)
    residual = (tokens.astype(jnp.float32) + mixer_out.astype(jnp.float32)).astype(jnp.bfloat16)
    expert_input = rms_rows(residual.astype(jnp.float32), channel_gain).astype(jnp.bfloat16)
    weight_norm = route_weights / lax.optimization_barrier(jnp.sum(route_weights, axis=1, keepdims=True)) * ROUTED_SCALE
    pair_ids = routes.reshape(N_EP, SEQ_DEV * TOP_K)
    order_pos = jnp.arange(SEQ_DEV * TOP_K, dtype=jnp.int32)
    earlier = (pair_ids[:, :, None] == pair_ids[:, None, :]) & (order_pos[None, :, None] > order_pos[None, None, :])
    slot_index = lax.optimization_barrier(jnp.sum(earlier.astype(jnp.int32), axis=2))
    block_ids = jnp.arange(N_EP, dtype=jnp.int32)[:, None]
    expert_rows = N_EP * CAP
    slot_flat = (pair_ids * expert_rows + block_ids * CAP + slot_index).reshape(-1).astype(jnp.int32)
    token_ids = jnp.repeat(jnp.arange(rows_total, dtype=jnp.int32), TOP_K)
    row_token = jnp.full((EXPERTS * expert_rows,), rows_total, jnp.int32).at[slot_flat].set(token_ids)
    row_weight = jnp.zeros((EXPERTS * expert_rows,), jnp.float32).at[slot_flat].set(weight_norm.reshape(-1))
    padded_rows = jnp.concatenate([expert_input, jnp.zeros((1, D), jnp.bfloat16)], axis=0)

    def one_expert(inputs):
        gate_mat, up_mat, down_mat, token_list = inputs
        chosen = padded_rows[token_list]
        gate_val = jnp.dot(chosen, gate_mat, preferred_element_type=jnp.float32)
        up_val = jnp.dot(chosen, up_mat, preferred_element_type=jnp.float32)
        hidden_act = (jax.nn.silu(gate_val) * up_val).astype(jnp.bfloat16)
        return group_sum(hidden_act, down_mat, N_TP)
    expert_out = lax.map(one_expert, (expert_gate, expert_up, expert_down, row_token.reshape(EXPERTS, expert_rows)))
    weighted = row_weight[:, None] * expert_out.reshape(-1, D).astype(jnp.float32)
    routed = jnp.zeros((rows_total + 1, D), jnp.float32).at[row_token].add(weighted)[:rows_total]
    shared_act = (jax.nn.silu(jnp.dot(expert_input, shared_gate, preferred_element_type=jnp.float32)) * jnp.dot(expert_input, shared_up, preferred_element_type=jnp.float32)).astype(jnp.bfloat16)
    shared_out = group_sum(shared_act, shared_down, N_TP)
    layer_out = (residual.astype(jnp.float32) + routed + shared_out.astype(jnp.float32)).astype(jnp.bfloat16)
    return (layer_out, next_state)
```

```python
import jax
import jax.numpy as jnp
from jax import lax
from jax.sharding import PartitionSpec as P

EPS = 1e-06
ROUTED_SCALE = 2.5


def sent_to_all(array, axis):
    copies = jnp.broadcast_to(array, (lax.axis_size(axis), *array.shape))
    return lax.all_to_all(copies, axis, split_axis=0, concat_axis=0, tiled=True)


def over_copies(array, axis):
    return sent_to_all(array, axis).astype(jnp.float32).sum(axis=0)


def in_blocks(array, dim, length):
    shape = array.shape
    tiles = array.reshape(*shape[:dim], length, shape[dim] // length, *shape[dim + 1 :])
    return jnp.moveaxis(tiles, dim, 0)


def sent_and_summed(array, axis, dim):
    length = lax.axis_size(axis)
    tiles = lax.all_to_all(in_blocks(array, dim, length), axis, 0, 0, tiled=True)
    return jnp.sum(tiles.astype(jnp.float32), axis=0)


def side_by_side(arrays, axis, dim, along):
    ends, at = ([], 0)
    for a in arrays[:-1]:
        at += a.shape[along]
        ends.append(at)
    both = jnp.concatenate(arrays, axis=along)
    return tuple(jnp.split(sent_and_summed(both, axis, dim), ends, axis=along))


def rms_rows(values, gain_vec):
    mean_square = jnp.mean(values * values, axis=-1, keepdims=True)
    return values * lax.rsqrt(mean_square + EPS) * gain_vec


def unit_heads(raw, heads, head_dim):
    shaped = raw.astype(jnp.float32).reshape(raw.shape[0], heads, head_dim)
    return shaped * lax.rsqrt(jnp.sum(shaped * shaped, axis=-1, keepdims=True) + EPS)


def per_device(
    tokens,
    delta_state,
    mixer_gain,
    query_weight,
    key_weight,
    value_weight,
    write_weight,
    decay_weight,
    decay_rate,
    decay_bias,
    head_gain,
    out_weight,
    channel_gain,
    routes,
    route_weights,
    expert_gate,
    expert_up,
    expert_down,
    shared_gate,
    shared_up,
    shared_down,
):
    seq_rows, model_width = tokens.shape
    heads, head_dim = (delta_state.shape[1], delta_state.shape[2])
    top_k = routes.shape[1]
    tp_count = lax.axis_size("tp")
    ep_count = lax.axis_size("ep")
    share_width = model_width // tp_count
    share_start = lax.axis_index("tp") * share_width
    exp_local = expert_gate.shape[0]
    expert_total = exp_local * ep_count
    pair_count = seq_rows * top_k
    parity = lax.axis_index("tp") % 2
    partner = [(i, i ^ 1) for i in range(tp_count)]
    normed = rms_rows(tokens.astype(jnp.float32), mixer_gain).astype(jnp.bfloat16)
    query_raw = jnp.dot(normed, query_weight, preferred_element_type=jnp.float32).astype(
        jnp.bfloat16
    )
    key_raw = jnp.dot(normed, key_weight, preferred_element_type=jnp.float32).astype(jnp.bfloat16)
    value_raw = jnp.dot(normed, value_weight, preferred_element_type=jnp.float32).astype(
        jnp.bfloat16
    )
    write_rate = jax.nn.sigmoid(jnp.dot(normed, write_weight, preferred_element_type=jnp.float32))
    decay_keep = jnp.exp(
        -decay_rate
        * jax.nn.softplus(
            jnp.dot(normed, decay_weight, preferred_element_type=jnp.float32) + decay_bias
        )
    )
    query_unit = unit_heads(query_raw, heads, head_dim) * head_dim ** (-0.5)
    key_unit = unit_heads(key_raw, heads, head_dim)
    value_vec = value_raw.astype(jnp.float32).reshape(seq_rows, heads, head_dim)
    held_state = decay_keep[:, :, None, None] * delta_state
    correction = value_vec - jnp.einsum(
        "rhkv,rhk->rhv", held_state, key_unit, precision=lax.Precision.HIGHEST
    )
    next_state = (
        held_state
        + write_rate[:, :, None, None] * key_unit[:, :, :, None] * correction[:, :, None, :]
    )
    readout = jnp.einsum("rhkv,rhk->rhv", next_state, query_unit, precision=lax.Precision.HIGHEST)
    head_out = rms_rows(readout, head_gain).astype(jnp.bfloat16).reshape(seq_rows, heads * head_dim)
    head_partial = jnp.dot(head_out, out_weight, preferred_element_type=jnp.float32)
    head_partial = head_partial.astype(jnp.bfloat16).astype(jnp.float32)
    mixer_out = over_copies(head_partial.astype(jnp.bfloat16), "tp").astype(jnp.bfloat16)
    gate_own, up_own, down_own = (expert_gate[0], expert_up[0], expert_down[0])
    gate_other = lax.ppermute(gate_own, "tp", partner)
    up_other = lax.ppermute(up_own, "tp", partner)
    down_other = lax.ppermute(down_own, "tp", partner)
    residual = (tokens.astype(jnp.float32) + mixer_out.astype(jnp.float32)).astype(jnp.bfloat16)
    expert_input = rms_rows(residual.astype(jnp.float32), channel_gain).astype(jnp.bfloat16)
    residual_share = lax.dynamic_slice_in_dim(residual, share_start, share_width, 1)
    weight_norm = route_weights / jnp.sum(route_weights, axis=1, keepdims=True) * ROUTED_SCALE
    shared_act = (
        jax.nn.silu(jnp.dot(expert_input, shared_gate, preferred_element_type=jnp.float32))
        * jnp.dot(expert_input, shared_up, preferred_element_type=jnp.float32)
    ).astype(jnp.bfloat16)
    shared_partial = jnp.dot(shared_act, shared_down, preferred_element_type=jnp.float32)
    shared_partial = shared_partial.astype(jnp.bfloat16).astype(jnp.float32)
    order_pos = jnp.arange(pair_count, dtype=jnp.int32)
    pair_ids = routes.reshape(pair_count)
    earlier = (pair_ids[:, None] == pair_ids[None, :]) & (order_pos[:, None] > order_pos[None, :])
    slot_index = jnp.sum(earlier.astype(jnp.int32), axis=1)
    expert_iota = jnp.arange(expert_total, dtype=jnp.int32)
    hit_table = (
        (expert_iota[:, None] == pair_ids[None, :]) & (slot_index[None, :] == parity)
    ).astype(jnp.float32)
    dispatch = jnp.sum(hit_table.reshape(expert_total, seq_rows, top_k), axis=2).astype(
        jnp.bfloat16
    )
    combine_mat = jnp.sum(
        (hit_table * weight_norm.reshape(1, pair_count)).reshape(expert_total, seq_rows, top_k),
        axis=2,
    )
    outgoing = jnp.dot(dispatch, expert_input, preferred_element_type=jnp.float32).astype(
        jnp.bfloat16
    )
    received = lax.all_to_all(
        outgoing.reshape(ep_count, 1, model_width), "ep", split_axis=0, concat_axis=0, tiled=True
    )
    rows = received.reshape(ep_count, model_width)
    down_part = jnp.zeros((ep_count, model_width), jnp.float32)
    for gate, up, down in (
        (gate_own, up_own, down_own),
        (gate_other, up_other, down_other),
    ):
        gate_val = jnp.dot(rows, gate, preferred_element_type=jnp.float32)
        up_val = jnp.dot(rows, up, preferred_element_type=jnp.float32)
        hidden_act = (jax.nn.silu(gate_val) * up_val).astype(jnp.bfloat16)
        down_part = down_part + jnp.dot(hidden_act, down, preferred_element_type=jnp.float32)
    homeward = down_part.astype(jnp.bfloat16).reshape(ep_count, 1, model_width)
    returned = lax.all_to_all(homeward, "ep", split_axis=0, concat_axis=0, tiled=True)
    routed = jnp.einsum(
        "ts,td->sd",
        combine_mat,
        returned.reshape(ep_count, model_width).astype(jnp.float32),
        precision=lax.Precision.HIGHEST,
    )
    share_sum = sent_and_summed((routed + shared_partial).astype(jnp.bfloat16), "tp", 1)
    layer_out = (residual_share.astype(jnp.float32) + share_sum).astype(jnp.bfloat16)
    return (layer_out, next_state)


def solution(mesh):
    return jax.shard_map(
        per_device,
        mesh=mesh,
        in_specs=(
            P("ep", None),
            P("ep", "tp", None, None),
            P(),
            P(None, "tp"),
            P(None, "tp"),
            P(None, "tp"),
            P(None, "tp"),
            P(None, "tp"),
            P("tp"),
            P("tp"),
            P(),
            P("tp", None),
            P(),
            P("ep", None),
            P("ep", None),
            P("ep", None, "tp"),
            P("ep", None, "tp"),
            P("ep", "tp", None),
            P(None, "tp"),
            P(None, "tp"),
            P("tp", None),
        ),
        out_specs=(P("ep", "tp"), P("ep", "tp", None, None)),
        check_vma=False,
    )
```

```python
import jax
import jax.numpy as jnp
from jax import lax
from jax.experimental import pallas as pl
from jax.experimental.pallas import tpu as pltpu
from jax.sharding import PartitionSpec as P

EPS = 1e-06
ROUTED_SCALE = 2.5


def rms_rows(values, gain_vec):
    mean_square = jnp.mean(values * values, axis=-1, keepdims=True)
    return values * lax.rsqrt(mean_square + EPS) * gain_vec


def unit_rows(raw):
    vals = raw.astype(jnp.bfloat16).astype(jnp.float32)
    return vals * lax.rsqrt(jnp.sum(vals * vals, axis=-1, keepdims=True) + EPS)


def columns_of(rows):
    pad = jnp.zeros((128 - rows.shape[0], rows.shape[1]), rows.dtype)
    return jnp.concatenate([rows, pad], axis=0).T


def mixer_kernel(
    tokens_ref,
    gain_ref,
    write_ref,
    decay_ref,
    head_gain_ref,
    rate_ref,
    bias_ref,
    query_hbm,
    key_hbm,
    value_hbm,
    state_hbm,
    out_weight_hbm,
    partial_ref,
    key_unit_ref,
    update_ref,
    keep_ref,
    query_v,
    key_v,
    value_v,
    state_v,
    out_weight_v,
    found_k,
    found_q,
    sems,
):
    seq_rows = tokens_ref.shape[0]
    half = seq_rows // 2
    copies = [
        pltpu.make_async_copy(query_hbm, query_v, sems.at[0]),
        pltpu.make_async_copy(key_hbm, key_v, sems.at[1]),
        pltpu.make_async_copy(value_hbm, value_v, sems.at[2]),
        pltpu.make_async_copy(
            state_hbm.at[pl.ds(0, half)], state_v.at[pl.ds(0, half)], sems.at[3]
        ),
        pltpu.make_async_copy(
            state_hbm.at[pl.ds(half, seq_rows - half)],
            state_v.at[pl.ds(half, seq_rows - half)],
            sems.at[4],
        ),
        pltpu.make_async_copy(out_weight_hbm, out_weight_v, sems.at[5]),
    ]
    for copy in copies:
        copy.start()
    normed = rms_rows(tokens_ref[...].astype(jnp.float32), gain_ref[...]).astype(jnp.bfloat16)
    wide = normed.astype(jnp.float32)
    write_logit = jnp.sum(wide * write_ref[...].astype(jnp.float32), axis=-1, keepdims=True)
    decay_logit = jnp.sum(wide * decay_ref[...].astype(jnp.float32), axis=-1, keepdims=True)
    write_rate = 1.0 / (1.0 + jnp.exp(-write_logit))
    biased = decay_logit + bias_ref[0]
    softplus = jnp.maximum(biased, 0.0) + jnp.log1p(jnp.exp(-jnp.abs(biased)))
    keep = jnp.exp(-rate_ref[0] * softplus)
    copies[0].wait()
    query_raw = jnp.dot(normed, query_v[...], preferred_element_type=jnp.float32)
    copies[1].wait()
    key_raw = jnp.dot(normed, key_v[...], preferred_element_type=jnp.float32)
    copies[2].wait()
    value_raw = jnp.dot(normed, value_v[...], preferred_element_type=jnp.float32)
    query_unit = unit_rows(query_raw) * query_raw.shape[1] ** (-0.5)
    key_unit = unit_rows(key_raw)
    value_vec = value_raw.astype(jnp.bfloat16).astype(jnp.float32)
    key_cols = columns_of(key_unit)
    query_cols = columns_of(query_unit)
    for row in range(seq_rows):
        if row == 0:
            copies[3].wait()
        if row == half:
            copies[4].wait()
        state = state_v[row]
        found_k[row : row + 1, :] = jnp.sum(
            state * key_cols[:, row : row + 1], axis=0, keepdims=True
        )
        found_q[row : row + 1, :] = jnp.sum(
            state * query_cols[:, row : row + 1], axis=0, keepdims=True
        )
    correction = value_vec - keep * found_k[...]
    overlap = jnp.sum(key_unit * query_unit, axis=-1, keepdims=True)
    update = write_rate * correction
    readout = keep * found_q[...] + overlap * update
    head_out = rms_rows(readout, head_gain_ref[...]).astype(jnp.bfloat16)
    copies[5].wait()
    partial = jnp.dot(head_out, out_weight_v[...], preferred_element_type=jnp.float32)
    partial = partial.astype(jnp.bfloat16)
    for copy_number in range(partial_ref.shape[0]):
        partial_ref[copy_number] = partial
    key_unit_ref[...] = key_unit
    update_ref[...] = update
    keep_ref[...] = jnp.broadcast_to(keep, keep_ref.shape)


def state_kernel(
    parity_ref,
    key_unit_ref,
    update_ref,
    keep_ref,
    routes_ref,
    weights_ref,
    state_hbm,
    gate_hbm,
    up_hbm,
    down_hbm,
    next_hbm,
    packed_hbm,
    dispatch_ref,
    combine_ref,
    state_v,
    next_v,
    sems,
):
    seq_rows = key_unit_ref.shape[0]
    width, hidden = gate_hbm.shape
    half = seq_rows // 2
    spans = [(0, half), (half, seq_rows - half)]
    loads = [
        pltpu.make_async_copy(
            state_hbm.at[pl.ds(at, size)], state_v.at[pl.ds(at, size)], sems.at[i]
        )
        for i, (at, size) in enumerate(spans)
    ]
    stores = [
        pltpu.make_async_copy(
            next_v.at[pl.ds(at, size)], next_hbm.at[pl.ds(at, size)], sems.at[2 + i]
        )
        for i, (at, size) in enumerate(spans)
    ]
    packs = [
        pltpu.make_async_copy(gate_hbm, packed_hbm.at[pl.ds(0, width)], sems.at[4]),
        pltpu.make_async_copy(up_hbm, packed_hbm.at[pl.ds(width, width)], sems.at[5]),
    ] + [
        pltpu.make_async_copy(
            down_hbm.at[:, pl.ds(j * hidden, hidden)],
            packed_hbm.at[pl.ds(2 * width + j * hidden, hidden)],
            sems.at[6 + j],
        )
        for j in range(width // hidden)
    ]
    for copy in loads + packs:
        copy.start()
    routes = routes_ref[...]
    weights = weights_ref[...]
    top_k = routes.shape[1]
    scale = weights / jnp.sum(weights, axis=1, keepdims=True) * ROUTED_SCALE
    expert_iota = lax.broadcasted_iota(jnp.int32, (seq_rows, 128), 1)
    named = jnp.zeros((seq_rows, 128), jnp.float32)
    mix = jnp.zeros((seq_rows, 128), jnp.float32)
    for route in range(top_k):
        hit = expert_iota == routes[:, route : route + 1]
        named = named + jnp.where(hit, 1.0, 0.0)
        mix = mix + jnp.where(hit, scale[:, route : route + 1], 0.0)
    row_a = lax.broadcasted_iota(jnp.int32, (seq_rows, seq_rows), 0)
    row_b = lax.broadcasted_iota(jnp.int32, (seq_rows, seq_rows), 1)
    below = jnp.where(row_b < row_a, 1.0, 0.0)
    earlier = jnp.dot(below, named, preferred_element_type=jnp.float32)
    slot = earlier.astype(jnp.int32)
    dispatch_ref[...] = jnp.where(slot == parity_ref[0], named, 0.0).astype(jnp.bfloat16)
    combine_ref[0] = jnp.where(slot == 0, mix, 0.0)
    combine_ref[1] = jnp.where(slot == 1, mix, 0.0)
    key_cols = columns_of(key_unit_ref[...])
    for part, (at, size) in enumerate(spans):
        loads[part].wait()
        for row in range(at, at + size):
            next_v[row] = (
                keep_ref[row : row + 1, :] * state_v[row]
                + key_cols[:, row : row + 1] * update_ref[row : row + 1, :]
            )
        stores[part].start()
    for copy in stores + packs:
        copy.wait()


def vmem():
    return pl.BlockSpec(memory_space=pltpu.VMEM)


def smem():
    return pl.BlockSpec(memory_space=pltpu.SMEM)


def anywhere():
    return pl.BlockSpec(memory_space=pl.ANY)


def per_device(
    tokens,
    delta_state,
    mixer_gain,
    query_weight,
    key_weight,
    value_weight,
    write_weight,
    decay_weight,
    decay_rate,
    decay_bias,
    head_gain,
    out_weight,
    channel_gain,
    routes,
    route_weights,
    expert_gate,
    expert_up,
    expert_down,
    shared_gate,
    shared_up,
    shared_down,
):
    seq_rows, model_width = tokens.shape
    head_dim = delta_state.shape[2]
    tp_count = lax.axis_size("tp")
    ep_count = lax.axis_size("ep")
    share_width = model_width // tp_count
    hidden = expert_gate.shape[2]
    tp_index = lax.axis_index("tp")
    parity = (tp_index % 2).astype(jnp.int32).reshape(1)
    f32, bf16 = jnp.float32, jnp.bfloat16
    state = delta_state.reshape(seq_rows, head_dim, head_dim)
    small = jax.ShapeDtypeStruct((seq_rows, head_dim), f32)
    partials, key_unit, update, keep = pl.pallas_call(
        mixer_kernel,
        out_shape=[
            jax.ShapeDtypeStruct((tp_count, seq_rows, model_width), bf16),
            small,
            small,
            small,
        ],
        in_specs=[vmem()] * 5 + [smem()] * 2 + [anywhere()] * 5,
        out_specs=[vmem()] * 4,
        scratch_shapes=[
            pltpu.VMEM((model_width, head_dim), bf16),
            pltpu.VMEM((model_width, head_dim), bf16),
            pltpu.VMEM((model_width, head_dim), bf16),
            pltpu.VMEM((seq_rows, head_dim, head_dim), f32),
            pltpu.VMEM((head_dim, model_width), bf16),
            pltpu.VMEM((seq_rows, head_dim), f32),
            pltpu.VMEM((seq_rows, head_dim), f32),
            pltpu.SemaphoreType.DMA((6,)),
        ],
    )(
        tokens,
        mixer_gain.reshape(1, model_width),
        write_weight.reshape(1, model_width),
        decay_weight.reshape(1, model_width),
        head_gain.reshape(1, head_dim),
        decay_rate,
        decay_bias,
        query_weight,
        key_weight,
        value_weight,
        state,
        out_weight,
    )
    gathered = lax.all_to_all(partials, "tp", 0, 0, tiled=True)
    next_state, packed, dispatch, combine = pl.pallas_call(
        state_kernel,
        out_shape=[
            jax.ShapeDtypeStruct((seq_rows, head_dim, head_dim), f32),
            jax.ShapeDtypeStruct((3 * model_width, hidden), bf16),
            jax.ShapeDtypeStruct((seq_rows, ep_count), bf16),
            jax.ShapeDtypeStruct((2, seq_rows, ep_count), f32),
        ],
        in_specs=[smem()] + [vmem()] * 5 + [anywhere()] * 4,
        out_specs=[anywhere()] * 2 + [vmem()] * 2,
        scratch_shapes=[
            pltpu.VMEM((seq_rows, head_dim, head_dim), f32),
            pltpu.VMEM((seq_rows, head_dim, head_dim), f32),
            pltpu.SemaphoreType.DMA((6 + model_width // hidden,)),
        ],
    )(
        parity,
        key_unit,
        update,
        keep,
        routes,
        route_weights,
        state,
        expert_gate[0],
        expert_up[0],
        expert_down[0],
    )
    other = lax.ppermute(packed, "tp", [(i, i ^ 1) for i in range(tp_count)])
    mixer_out = jnp.sum(gathered.astype(f32), axis=0).astype(bf16)
    residual = (tokens.astype(f32) + mixer_out.astype(f32)).astype(bf16)
    expert_input = rms_rows(residual.astype(f32), channel_gain).astype(bf16)
    outgoing = lax.dot_general(
        dispatch, expert_input, (((0,), (0,)), ((), ())), preferred_element_type=f32
    ).astype(bf16)
    received = lax.all_to_all(
        outgoing.reshape(ep_count, 2, model_width // 2), "ep", 0, 0, tiled=True
    )
    shared_act = (
        jax.nn.silu(jnp.dot(expert_input, shared_gate, preferred_element_type=f32))
        * jnp.dot(expert_input, shared_up, preferred_element_type=f32)
    ).astype(bf16)
    shared_partial = jnp.dot(shared_act, shared_down, preferred_element_type=f32).astype(bf16)
    rows = received.reshape(ep_count, model_width)
    down_part = jnp.zeros((ep_count, model_width), f32)
    for pack in (packed, other):
        gate_val = jnp.dot(rows, pack[:model_width], preferred_element_type=f32)
        up_val = jnp.dot(rows, pack[model_width : 2 * model_width], preferred_element_type=f32)
        hidden_act = (jax.nn.silu(gate_val) * up_val).astype(bf16)
        down = pack[2 * model_width :].reshape(model_width // hidden, hidden, hidden)
        down_part = down_part + jnp.einsum(
            "rf,jfd->rjd", hidden_act, down, preferred_element_type=f32
        ).reshape(ep_count, model_width)
    both = jnp.concatenate([down_part.astype(bf16), shared_partial], axis=0)
    blocks = both.reshape(ep_count + seq_rows, tp_count, share_width).transpose(1, 0, 2)
    parts = lax.all_to_all(blocks, "tp", 0, 0, tiled=True).astype(f32)
    expert_share = jnp.stack(
        [parts[0, :ep_count] + parts[2, :ep_count], parts[1, :ep_count] + parts[3, :ep_count]],
        axis=1,
    ).astype(bf16)
    shared_out = jnp.sum(parts[:, ep_count:], axis=0).astype(bf16)
    returned = lax.all_to_all(expert_share, "ep", 0, 0, tiled=True)
    routed = jnp.einsum(
        "cse,ecd->sd", combine, returned.astype(f32), precision=lax.Precision.HIGHEST
    )
    residual_share = lax.dynamic_slice_in_dim(residual, tp_index * share_width, share_width, 1)
    layer_out = (residual_share.astype(f32) + routed + shared_out.astype(f32)).astype(bf16)
    return (layer_out, next_state.reshape(delta_state.shape))


def solution(mesh):
    return jax.shard_map(
        per_device,
        mesh=mesh,
        in_specs=(
            P("ep", None),
            P("ep", "tp", None, None),
            P(),
            P(None, "tp"),
            P(None, "tp"),
            P(None, "tp"),
            P(None, "tp"),
            P(None, "tp"),
            P("tp"),
            P("tp"),
            P(),
            P("tp", None),
            P(),
            P("ep", None),
            P("ep", None),
            P("ep", None, "tp"),
            P("ep", None, "tp"),
            P("ep", "tp", None),
            P(None, "tp"),
            P(None, "tp"),
            P("tp", None),
        ),
        out_specs=(P("ep", "tp"), P("ep", "tp", None, None)),
        check_vma=False,
    )
```

```python
import jax
import jax.numpy as jnp
from jax import lax
from jax.experimental import pallas as pl
from jax.experimental.pallas import tpu as pltpu
from jax.sharding import PartitionSpec as P

EPS = 1e-06
ROUTED_SCALE = 2.5


def rms_rows(values, gain_vec):
    mean_square = jnp.mean(values * values, axis=-1, keepdims=True)
    return values * lax.rsqrt(mean_square + EPS) * gain_vec


def unit_rows(raw):
    vals = raw.astype(jnp.bfloat16).astype(jnp.float32)
    return vals * lax.rsqrt(jnp.sum(vals * vals, axis=-1, keepdims=True) + EPS)


def columns_of(rows):
    pad = jnp.zeros((128 - rows.shape[0], rows.shape[1]), rows.dtype)
    return jnp.concatenate([rows, pad], axis=0).T


def mixer_kernel(
    tokens_ref,
    gain_ref,
    write_ref,
    decay_ref,
    head_gain_ref,
    rate_ref,
    bias_ref,
    query_hbm,
    key_hbm,
    value_hbm,
    state_hbm,
    out_weight_hbm,
    partial_ref,
    key_unit_ref,
    update_ref,
    keep_ref,
    query_v,
    key_v,
    value_v,
    state_v,
    out_weight_v,
    found_k,
    found_q,
    sems,
):
    seq_rows = tokens_ref.shape[0]
    half = seq_rows // 2
    copies = [
        pltpu.make_async_copy(query_hbm, query_v, sems.at[0]),
        pltpu.make_async_copy(key_hbm, key_v, sems.at[1]),
        pltpu.make_async_copy(value_hbm, value_v, sems.at[2]),
        pltpu.make_async_copy(
            state_hbm.at[pl.ds(0, half)], state_v.at[pl.ds(0, half)], sems.at[3]
        ),
        pltpu.make_async_copy(
            state_hbm.at[pl.ds(half, seq_rows - half)],
            state_v.at[pl.ds(half, seq_rows - half)],
            sems.at[4],
        ),
        pltpu.make_async_copy(out_weight_hbm, out_weight_v, sems.at[5]),
    ]
    for copy in copies:
        copy.start()
    normed = rms_rows(tokens_ref[...].astype(jnp.float32), gain_ref[...]).astype(jnp.bfloat16)
    wide = normed.astype(jnp.float32)
    write_logit = jnp.sum(wide * write_ref[...].astype(jnp.float32), axis=-1, keepdims=True)
    decay_logit = jnp.sum(wide * decay_ref[...].astype(jnp.float32), axis=-1, keepdims=True)
    write_rate = 1.0 / (1.0 + jnp.exp(-write_logit))
    biased = decay_logit + bias_ref[0]
    softplus = jnp.maximum(biased, 0.0) + jnp.log1p(jnp.exp(-jnp.abs(biased)))
    keep = jnp.exp(-rate_ref[0] * softplus)
    copies[0].wait()
    query_raw = jnp.dot(normed, query_v[...], preferred_element_type=jnp.float32)
    copies[1].wait()
    key_raw = jnp.dot(normed, key_v[...], preferred_element_type=jnp.float32)
    copies[2].wait()
    value_raw = jnp.dot(normed, value_v[...], preferred_element_type=jnp.float32)
    query_unit = unit_rows(query_raw) * query_raw.shape[1] ** (-0.5)
    key_unit = unit_rows(key_raw)
    value_vec = value_raw.astype(jnp.bfloat16).astype(jnp.float32)
    key_cols = columns_of(key_unit)
    query_cols = columns_of(query_unit)
    for row in range(seq_rows):
        if row == 0:
            copies[3].wait()
        if row == half:
            copies[4].wait()
        state = state_v[row]
        found_k[row : row + 1, :] = jnp.sum(
            state * key_cols[:, row : row + 1], axis=0, keepdims=True
        )
        found_q[row : row + 1, :] = jnp.sum(
            state * query_cols[:, row : row + 1], axis=0, keepdims=True
        )
    correction = value_vec - keep * found_k[...]
    overlap = jnp.sum(key_unit * query_unit, axis=-1, keepdims=True)
    update = write_rate * correction
    readout = keep * found_q[...] + overlap * update
    head_out = rms_rows(readout, head_gain_ref[...]).astype(jnp.bfloat16)
    copies[5].wait()
    partial = jnp.dot(head_out, out_weight_v[...], preferred_element_type=jnp.float32)
    partial = partial.astype(jnp.bfloat16)
    for copy_number in range(partial_ref.shape[0]):
        partial_ref[copy_number] = partial
    key_unit_ref[...] = key_unit
    update_ref[...] = update
    keep_ref[...] = jnp.broadcast_to(keep, keep_ref.shape)


def tables_kernel(
    parity_ref,
    routes_ref,
    weights_ref,
    gate_hbm,
    up_hbm,
    down_hbm,
    packed_hbm,
    dispatch_ref,
    combine_ref,
    packed_v,
    sems,
):
    width, hidden = gate_hbm.shape
    loads = [
        pltpu.make_async_copy(gate_hbm, packed_v.at[pl.ds(0, width)], sems.at[0]),
        pltpu.make_async_copy(up_hbm, packed_v.at[pl.ds(width, width)], sems.at[1]),
    ] + [
        pltpu.make_async_copy(
            down_hbm.at[:, pl.ds(j * hidden, hidden)],
            packed_v.at[pl.ds(2 * width + j * hidden, hidden)],
            sems.at[2 + j],
        )
        for j in range(width // hidden)
    ]
    for copy in loads:
        copy.start()
    top_k, seq_rows = routes_ref.shape
    routes = columns_of(routes_ref[...].astype(jnp.float32))[:seq_rows].astype(jnp.int32)
    weights = columns_of(weights_ref[...])[:seq_rows]
    scale = weights / jnp.sum(weights, axis=1, keepdims=True) * ROUTED_SCALE
    expert_iota = lax.broadcasted_iota(jnp.int32, (seq_rows, 128), 1)
    named = jnp.zeros((seq_rows, 128), jnp.float32)
    mix = jnp.zeros((seq_rows, 128), jnp.float32)
    for route in range(top_k):
        hit = expert_iota == routes[:, route : route + 1]
        named = named + jnp.where(hit, 1.0, 0.0)
        mix = mix + jnp.where(hit, scale[:, route : route + 1], 0.0)
    row_a = lax.broadcasted_iota(jnp.int32, (seq_rows, seq_rows), 0)
    row_b = lax.broadcasted_iota(jnp.int32, (seq_rows, seq_rows), 1)
    below = jnp.where(row_b < row_a, 1.0, 0.0)
    earlier = jnp.dot(below, named, preferred_element_type=jnp.float32)
    slot = earlier.astype(jnp.int32)
    dispatch_ref[...] = jnp.where(slot == parity_ref[0], named, 0.0).astype(jnp.bfloat16)
    combine_ref[0] = jnp.where(slot == 0, mix, 0.0)
    combine_ref[1] = jnp.where(slot == 1, mix, 0.0)
    for copy in loads:
        copy.wait()
    store = pltpu.make_async_copy(packed_v, packed_hbm, sems.at[0])
    store.start()
    store.wait()


def state_kernel(
    key_unit_ref,
    update_ref,
    keep_ref,
    state_hbm,
    next_hbm,
    state_v,
    next_v,
    sems,
):
    seq_rows = key_unit_ref.shape[0]
    half = seq_rows // 2
    spans = [(0, half), (half, seq_rows - half)]
    loads = [
        pltpu.make_async_copy(
            state_hbm.at[pl.ds(at, size)], state_v.at[pl.ds(at, size)], sems.at[i]
        )
        for i, (at, size) in enumerate(spans)
    ]
    stores = [
        pltpu.make_async_copy(
            next_v.at[pl.ds(at, size)], next_hbm.at[pl.ds(at, size)], sems.at[2 + i]
        )
        for i, (at, size) in enumerate(spans)
    ]
    for copy in loads:
        copy.start()
    key_cols = columns_of(key_unit_ref[...])
    for part, (at, size) in enumerate(spans):
        loads[part].wait()
        for row in range(at, at + size):
            next_v[row] = (
                keep_ref[row : row + 1, :] * state_v[row]
                + key_cols[:, row : row + 1] * update_ref[row : row + 1, :]
            )
        stores[part].start()
    for copy in stores:
        copy.wait()


def vmem():
    return pl.BlockSpec(memory_space=pltpu.VMEM)


def smem():
    return pl.BlockSpec(memory_space=pltpu.SMEM)


def anywhere():
    return pl.BlockSpec(memory_space=pl.ANY)


def per_device(
    tokens,
    delta_state,
    mixer_gain,
    query_weight,
    key_weight,
    value_weight,
    write_weight,
    decay_weight,
    decay_rate,
    decay_bias,
    head_gain,
    out_weight,
    channel_gain,
    routes,
    route_weights,
    expert_gate,
    expert_up,
    expert_down,
    shared_gate,
    shared_up,
    shared_down,
):
    seq_rows, model_width = tokens.shape
    head_dim = delta_state.shape[2]
    tp_count = lax.axis_size("tp")
    ep_count = lax.axis_size("ep")
    share_width = model_width // tp_count
    hidden = expert_gate.shape[2]
    tp_index = lax.axis_index("tp")
    parity = (tp_index % 2).astype(jnp.int32).reshape(1)
    f32, bf16 = jnp.float32, jnp.bfloat16
    state = delta_state.reshape(seq_rows, head_dim, head_dim)
    small = jax.ShapeDtypeStruct((seq_rows, head_dim), f32)
    partials, key_unit, update, keep = pl.pallas_call(
        mixer_kernel,
        out_shape=[
            jax.ShapeDtypeStruct((tp_count, seq_rows, model_width), bf16),
            small,
            small,
            small,
        ],
        in_specs=[vmem()] * 5 + [smem()] * 2 + [anywhere()] * 5,
        out_specs=[vmem()] * 4,
        scratch_shapes=[
            pltpu.VMEM((model_width, head_dim), bf16),
            pltpu.VMEM((model_width, head_dim), bf16),
            pltpu.VMEM((model_width, head_dim), bf16),
            pltpu.VMEM((seq_rows, head_dim, head_dim), f32),
            pltpu.VMEM((head_dim, model_width), bf16),
            pltpu.VMEM((seq_rows, head_dim), f32),
            pltpu.VMEM((seq_rows, head_dim), f32),
            pltpu.SemaphoreType.DMA((6,)),
        ],
    )(
        tokens,
        mixer_gain.reshape(1, model_width),
        write_weight.reshape(1, model_width),
        decay_weight.reshape(1, model_width),
        head_gain.reshape(1, head_dim),
        decay_rate,
        decay_bias,
        query_weight,
        key_weight,
        value_weight,
        state,
        out_weight,
    )
    gathered = lax.all_to_all(partials, "tp", 0, 0, tiled=True)
    packed, dispatch, combine = pl.pallas_call(
        tables_kernel,
        out_shape=[
            jax.ShapeDtypeStruct((3 * model_width, hidden), bf16),
            jax.ShapeDtypeStruct((seq_rows, ep_count), bf16),
            jax.ShapeDtypeStruct((2, seq_rows, ep_count), f32),
        ],
        in_specs=[smem()] + [vmem()] * 2 + [anywhere()] * 3,
        out_specs=[anywhere()] + [vmem()] * 2,
        scratch_shapes=[
            pltpu.VMEM((3 * model_width, hidden), bf16),
            pltpu.SemaphoreType.DMA((2 + model_width // hidden,)),
        ],
    )(
        parity,
        routes.T,
        route_weights.T,
        expert_gate[0],
        expert_up[0],
        expert_down[0],
    )
    next_state = pl.pallas_call(
        state_kernel,
        out_shape=jax.ShapeDtypeStruct((seq_rows, head_dim, head_dim), f32),
        in_specs=[vmem()] * 3 + [anywhere()],
        out_specs=anywhere(),
        scratch_shapes=[
            pltpu.VMEM((seq_rows, head_dim, head_dim), f32),
            pltpu.VMEM((seq_rows, head_dim, head_dim), f32),
            pltpu.SemaphoreType.DMA((4,)),
        ],
    )(key_unit, update, keep, state)
    other = lax.ppermute(packed, "tp", [(i, i ^ 1) for i in range(tp_count)])
    mixer_out = jnp.sum(gathered.astype(f32), axis=0).astype(bf16)
    residual = (tokens.astype(f32) + mixer_out.astype(f32)).astype(bf16)
    expert_input = rms_rows(residual.astype(f32), channel_gain).astype(bf16)
    outgoing = lax.dot_general(
        dispatch, expert_input, (((0,), (0,)), ((), ())), preferred_element_type=f32
    ).astype(bf16)
    received = lax.all_to_all(
        outgoing.reshape(ep_count, 2, model_width // 2), "ep", 0, 0, tiled=True
    )
    shared_act = (
        jax.nn.silu(jnp.dot(expert_input, shared_gate, preferred_element_type=f32))
        * jnp.dot(expert_input, shared_up, preferred_element_type=f32)
    ).astype(bf16)
    shared_partial = jnp.dot(shared_act, shared_down, preferred_element_type=f32).astype(bf16)
    rows = received.reshape(ep_count, model_width)
    down_part = jnp.zeros((ep_count, model_width), f32)
    for pack in (packed, other):
        gate_val = jnp.dot(rows, pack[:model_width], preferred_element_type=f32)
        up_val = jnp.dot(rows, pack[model_width : 2 * model_width], preferred_element_type=f32)
        hidden_act = (jax.nn.silu(gate_val) * up_val).astype(bf16)
        down = pack[2 * model_width :].reshape(model_width // hidden, hidden, hidden)
        down_part = down_part + jnp.einsum(
            "rf,jfd->rjd", hidden_act, down, preferred_element_type=f32
        ).reshape(ep_count, model_width)
    both = jnp.concatenate([down_part.astype(bf16), shared_partial], axis=0)
    blocks = both.reshape(ep_count + seq_rows, tp_count, share_width).transpose(1, 0, 2)
    parts = lax.all_to_all(blocks, "tp", 0, 0, tiled=True).astype(f32)
    expert_share = jnp.stack(
        [parts[0, :ep_count] + parts[2, :ep_count], parts[1, :ep_count] + parts[3, :ep_count]],
        axis=1,
    ).astype(bf16)
    shared_out = jnp.sum(parts[:, ep_count:], axis=0).astype(bf16)
    returned = lax.all_to_all(expert_share, "ep", 0, 0, tiled=True)
    routed = jnp.einsum(
        "cse,ecd->sd", combine, returned.astype(f32), precision=lax.Precision.HIGHEST
    )
    residual_share = lax.dynamic_slice_in_dim(residual, tp_index * share_width, share_width, 1)
    layer_out = (residual_share.astype(f32) + routed + shared_out.astype(f32)).astype(bf16)
    return (layer_out, next_state.reshape(delta_state.shape))


def solution(mesh):
    return jax.shard_map(
        per_device,
        mesh=mesh,
        in_specs=(
            P("ep", None),
            P("ep", "tp", None, None),
            P(),
            P(None, "tp"),
            P(None, "tp"),
            P(None, "tp"),
            P(None, "tp"),
            P(None, "tp"),
            P("tp"),
            P("tp"),
            P(),
            P("tp", None),
            P(),
            P("ep", None),
            P("ep", None),
            P("ep", None, "tp"),
            P("ep", None, "tp"),
            P("ep", "tp", None),
            P(None, "tp"),
            P(None, "tp"),
            P("tp", None),
        ),
        out_specs=(P("ep", "tp"), P("ep", "tp", None, None)),
        check_vma=False,
    )
```

```python
import jax
import jax.numpy as jnp
from jax import lax
from jax.experimental import pallas as pl
from jax.experimental.pallas import tpu as pltpu
from jax.sharding import PartitionSpec as P

EPS = 1e-06
ROUTED_SCALE = 2.5


def rms_rows(values, gain_vec):
    mean_square = jnp.mean(values * values, axis=-1, keepdims=True)
    return values * lax.rsqrt(mean_square + EPS) * gain_vec


def unit_rows(raw):
    vals = raw.astype(jnp.bfloat16).astype(jnp.float32)
    return vals * lax.rsqrt(jnp.sum(vals * vals, axis=-1, keepdims=True) + EPS)


def columns_of(rows):
    pad = jnp.zeros((128 - rows.shape[0], rows.shape[1]), rows.dtype)
    return jnp.concatenate([rows, pad], axis=0).T


def mixer_kernel(
    parity_ref,
    tokens_hbm,
    gain_hbm,
    write_hbm,
    decay_hbm,
    head_gain_hbm,
    rate_hbm,
    bias_hbm,
    routes_hbm,
    weights_hbm,
    query_hbm,
    key_hbm,
    value_hbm,
    state_hbm,
    out_weight_hbm,
    gate_hbm,
    up_hbm,
    down_hbm,
    partial_ref,
    key_unit_ref,
    update_ref,
    keep_ref,
    dispatch_ref,
    combine_ref,
    packed_hbm,
    tokens_v,
    gain_v,
    write_v,
    decay_v,
    head_gain_v,
    rate_v,
    bias_v,
    routes_v,
    weights_v,
    query_v,
    key_v,
    value_v,
    state_v,
    out_weight_v,
    packed_v,
    found_k,
    found_q,
    sems,
):
    seq_rows = tokens_hbm.shape[0]
    width, hidden = gate_hbm.shape
    half = seq_rows // 2
    pairs = [
        (tokens_hbm, tokens_v),
        (gain_hbm, gain_v),
        (write_hbm, write_v),
        (decay_hbm, decay_v),
        (rate_hbm, rate_v),
        (bias_hbm, bias_v),
        (query_hbm, query_v),
        (key_hbm, key_v),
        (value_hbm, value_v),
        (state_hbm.at[pl.ds(0, half)], state_v.at[pl.ds(0, half)]),
        (
            state_hbm.at[pl.ds(half, seq_rows - half)],
            state_v.at[pl.ds(half, seq_rows - half)],
        ),
        (routes_hbm, routes_v),
        (weights_hbm, weights_v),
        (head_gain_hbm, head_gain_v),
        (out_weight_hbm, out_weight_v),
        (gate_hbm, packed_v.at[pl.ds(0, width)]),
        (up_hbm, packed_v.at[pl.ds(width, width)]),
    ] + [
        (
            down_hbm.at[:, pl.ds(j * hidden, hidden)],
            packed_v.at[pl.ds(2 * width + j * hidden, hidden)],
        )
        for j in range(width // hidden)
    ]
    loads = [pltpu.make_async_copy(src, dst, sems.at[i]) for i, (src, dst) in enumerate(pairs)]
    for copy in loads:
        copy.start()
    for copy in loads[:6]:
        copy.wait()
    normed = rms_rows(tokens_v[...].astype(jnp.float32), gain_v[...]).astype(jnp.bfloat16)
    wide = normed.astype(jnp.float32)
    write_logit = jnp.sum(wide * write_v[...].astype(jnp.float32), axis=-1, keepdims=True)
    decay_logit = jnp.sum(wide * decay_v[...].astype(jnp.float32), axis=-1, keepdims=True)
    write_rate = 1.0 / (1.0 + jnp.exp(-write_logit))
    biased = decay_logit + bias_v[0]
    softplus = jnp.maximum(biased, 0.0) + jnp.log1p(jnp.exp(-jnp.abs(biased)))
    keep = jnp.exp(-rate_v[0] * softplus)
    loads[6].wait()
    query_raw = jnp.dot(normed, query_v[...], preferred_element_type=jnp.float32)
    loads[7].wait()
    key_raw = jnp.dot(normed, key_v[...], preferred_element_type=jnp.float32)
    loads[8].wait()
    value_raw = jnp.dot(normed, value_v[...], preferred_element_type=jnp.float32)
    query_unit = unit_rows(query_raw) * query_raw.shape[1] ** (-0.5)
    key_unit = unit_rows(key_raw)
    value_vec = value_raw.astype(jnp.bfloat16).astype(jnp.float32)
    key_cols = columns_of(key_unit)
    query_cols = columns_of(query_unit)
    for row in range(seq_rows):
        if row == 0:
            loads[9].wait()
        if row == half:
            loads[10].wait()
        state = state_v[row]
        found_k[row : row + 1, :] = jnp.sum(
            state * key_cols[:, row : row + 1], axis=0, keepdims=True
        )
        found_q[row : row + 1, :] = jnp.sum(
            state * query_cols[:, row : row + 1], axis=0, keepdims=True
        )
    for copy in loads[11:14]:
        copy.wait()
    correction = value_vec - keep * found_k[...]
    overlap = jnp.sum(key_unit * query_unit, axis=-1, keepdims=True)
    update = write_rate * correction
    readout = keep * found_q[...] + overlap * update
    head_out = rms_rows(readout, head_gain_v[...]).astype(jnp.bfloat16)
    loads[14].wait()
    partial = jnp.dot(head_out, out_weight_v[...], preferred_element_type=jnp.float32)
    partial = partial.astype(jnp.bfloat16)
    for copy_number in range(partial_ref.shape[0]):
        partial_ref[copy_number] = partial
    for copy in loads[15:]:
        copy.wait()
    store = pltpu.make_async_copy(packed_v, packed_hbm, sems.at[0])
    store.start()
    key_unit_ref[...] = key_unit
    update_ref[...] = update
    keep_ref[...] = jnp.broadcast_to(keep, keep_ref.shape)
    routes = columns_of(routes_v[...].astype(jnp.float32))[:seq_rows].astype(jnp.int32)
    weights = columns_of(weights_v[...])[:seq_rows]
    scale = weights / jnp.sum(weights, axis=1, keepdims=True) * ROUTED_SCALE
    expert_iota = lax.broadcasted_iota(jnp.int32, (seq_rows, 128), 1)
    named = jnp.zeros((seq_rows, 128), jnp.float32)
    mix = jnp.zeros((seq_rows, 128), jnp.float32)
    for route in range(routes_hbm.shape[0]):
        hit = expert_iota == routes[:, route : route + 1]
        named = named + jnp.where(hit, 1.0, 0.0)
        mix = mix + jnp.where(hit, scale[:, route : route + 1], 0.0)
    row_a = lax.broadcasted_iota(jnp.int32, (seq_rows, seq_rows), 0)
    row_b = lax.broadcasted_iota(jnp.int32, (seq_rows, seq_rows), 1)
    below = jnp.where(row_b < row_a, 1.0, 0.0)
    earlier = jnp.dot(below, named, preferred_element_type=jnp.float32)
    slot = earlier.astype(jnp.int32)
    dispatch_ref[...] = jnp.where(slot == parity_ref[0], named, 0.0).astype(jnp.bfloat16)
    combine_ref[0] = jnp.where(slot == 0, mix, 0.0)
    combine_ref[1] = jnp.where(slot == 1, mix, 0.0)
    store.wait()


def rows_kernel(
    gathered_ref,
    tokens_ref,
    gain_ref,
    dispatch_ref,
    residual_ref,
    input_ref,
    rows_ref,
    wide_v,
):
    mixed = jnp.sum(gathered_ref[...].astype(jnp.float32), axis=0)
    mixed = mixed.astype(jnp.bfloat16).astype(jnp.float32)
    residual = (tokens_ref[...].astype(jnp.float32) + mixed).astype(jnp.bfloat16)
    inputs = rms_rows(residual.astype(jnp.float32), gain_ref[...]).astype(jnp.bfloat16)
    residual_ref[...] = residual
    input_ref[...] = inputs
    experts = dispatch_ref.shape[1]
    picked = lax.dot_general(
        dispatch_ref[...], inputs, (((0,), (0,)), ((), ())), preferred_element_type=jnp.float32
    )
    lanes = inputs.shape[1] // 128
    for lane in range(lanes):
        wide_v[pl.ds(lane, experts, stride=lanes), :] = picked[:, lane * 128 : (lane + 1) * 128]
    rows_ref[...] = wide_v[...].astype(jnp.bfloat16)


def expert_kernel(
    rows_ref,
    own_ref,
    other_ref,
    shared_ref,
    blocks_ref,
    wide_v,
    rows_v,
):
    lanes = 8
    experts = rows_ref.shape[0] // lanes
    width = lanes * 128
    wide_v[...] = rows_ref[...].astype(jnp.float32)
    for lane in range(lanes):
        rows_v[:, lane * 128 : (lane + 1) * 128] = wide_v[
            pl.ds(lane, experts, stride=lanes), :
        ].astype(jnp.bfloat16)
    rows = rows_v[...]
    acts = []
    for pack_ref in (own_ref, other_ref):
        gate = jnp.dot(rows, pack_ref[:width], preferred_element_type=jnp.float32)
        up = jnp.dot(rows, pack_ref[width : 2 * width], preferred_element_type=jnp.float32)
        acts.append((gate / (1.0 + jnp.exp(-gate)) * up).astype(jnp.bfloat16))
    parts = blocks_ref.shape[0]
    share = width // parts
    for j in range(lanes):
        at = 2 * width + j * 128
        down = jnp.dot(acts[0], own_ref[at : at + 128], preferred_element_type=jnp.float32)
        down += jnp.dot(acts[1], other_ref[at : at + 128], preferred_element_type=jnp.float32)
        col = j * 128 % share
        blocks_ref[j * 128 // share, :experts, col : col + 128] = down.astype(jnp.bfloat16)
    for part in range(parts):
        blocks_ref[part, experts:, :] = shared_ref[:, part * share : (part + 1) * share]


def share_kernel(parts_ref, rows_ref, shared_ref, wide_v):
    share = parts_ref.shape[2]
    seq_rows = shared_ref.shape[0]
    experts = parts_ref.shape[1] - seq_rows
    quads = rows_ref.shape[0] // experts
    chunks = share // 128
    for slot in range(2):
        total = parts_ref[slot, :experts, :].astype(jnp.float32)
        total += parts_ref[slot + 2, :experts, :].astype(jnp.float32)
        for chunk in range(chunks):
            wide_v[pl.ds(slot * chunks + chunk, experts, stride=quads), :] = total[
                :, chunk * 128 : (chunk + 1) * 128
            ]
    rows_ref[...] = wide_v[...].astype(jnp.bfloat16)
    shared = jnp.sum(parts_ref[:, experts:, :].astype(jnp.float32), axis=0)
    shared_ref[...] = shared.astype(jnp.bfloat16).astype(jnp.float32)


def final_kernel(
    index_ref, rows_ref, combine_ref, residual_ref, shared_ref, out_ref, wide_v
):
    share = out_ref.shape[1]
    chunks = share // 128
    experts = combine_ref.shape[2]
    quads = rows_ref.shape[0] // experts
    wide_v[...] = rows_ref[...].astype(jnp.float32)
    at = pl.multiple_of(index_ref[0] * share, share)
    base = residual_ref[:, pl.ds(at, share)].astype(jnp.float32) + shared_ref[...]
    for chunk in range(chunks):
        routed = base[:, chunk * 128 : (chunk + 1) * 128]
        for slot in range(2):
            rows = wide_v[pl.ds(slot * chunks + chunk, experts, stride=quads), :]
            routed += jnp.dot(
                combine_ref[slot],
                rows,
                preferred_element_type=jnp.float32,
                precision=lax.Precision.HIGHEST,
            )
        out_ref[:, chunk * 128 : (chunk + 1) * 128] = routed.astype(jnp.bfloat16)


def state_kernel(
    key_unit_ref,
    update_ref,
    keep_ref,
    state_hbm,
    next_hbm,
    state_v,
    next_v,
    sems,
):
    seq_rows = key_unit_ref.shape[0]
    half = seq_rows // 2
    spans = [(0, half), (half, seq_rows - half)]
    loads = [
        pltpu.make_async_copy(
            state_hbm.at[pl.ds(at, size)], state_v.at[pl.ds(at, size)], sems.at[i]
        )
        for i, (at, size) in enumerate(spans)
    ]
    stores = [
        pltpu.make_async_copy(
            next_v.at[pl.ds(at, size)], next_hbm.at[pl.ds(at, size)], sems.at[2 + i]
        )
        for i, (at, size) in enumerate(spans)
    ]
    for copy in loads:
        copy.start()
    key_cols = columns_of(key_unit_ref[...])
    for part, (at, size) in enumerate(spans):
        loads[part].wait()
        for row in range(at, at + size):
            next_v[row] = (
                keep_ref[row : row + 1, :] * state_v[row]
                + key_cols[:, row : row + 1] * update_ref[row : row + 1, :]
            )
        stores[part].start()
    for copy in stores:
        copy.wait()


def vmem():
    return pl.BlockSpec(memory_space=pltpu.VMEM)


def smem():
    return pl.BlockSpec(memory_space=pltpu.SMEM)


def anywhere():
    return pl.BlockSpec(memory_space=pl.ANY)


def in_vmem(array):
    return pltpu.with_memory_space_constraint(array, pltpu.VMEM)


def per_device(
    tokens,
    delta_state,
    mixer_gain,
    query_weight,
    key_weight,
    value_weight,
    write_weight,
    decay_weight,
    decay_rate,
    decay_bias,
    head_gain,
    out_weight,
    channel_gain,
    routes,
    route_weights,
    expert_gate,
    expert_up,
    expert_down,
    shared_gate,
    shared_up,
    shared_down,
):
    seq_rows, model_width = tokens.shape
    head_dim = delta_state.shape[2]
    tp_count = lax.axis_size("tp")
    ep_count = lax.axis_size("ep")
    share_width = model_width // tp_count
    hidden = expert_gate.shape[2]
    tp_index = lax.axis_index("tp")
    parity = (tp_index % 2).astype(jnp.int32).reshape(1)
    f32, bf16 = jnp.float32, jnp.bfloat16
    state = delta_state.reshape(seq_rows, head_dim, head_dim)
    small = pltpu.VMEM((seq_rows, head_dim), f32)
    partials, key_unit, update, keep, dispatch, combine, packed = pl.pallas_call(
        mixer_kernel,
        out_shape=[
            jax.ShapeDtypeStruct((tp_count, seq_rows, model_width), bf16),
            small,
            small,
            small,
            pltpu.VMEM((seq_rows, ep_count), bf16),
            pltpu.VMEM((2, seq_rows, ep_count), f32),
            jax.ShapeDtypeStruct((3 * model_width, hidden), bf16),
        ],
        in_specs=[smem()] + [anywhere()] * 17,
        out_specs=[vmem()] * 6 + [anywhere()],
        scratch_shapes=[
            pltpu.VMEM((seq_rows, model_width), bf16),
            pltpu.VMEM((1, model_width), f32),
            pltpu.VMEM((1, model_width), bf16),
            pltpu.VMEM((1, model_width), bf16),
            pltpu.VMEM((1, head_dim), f32),
            pltpu.SMEM((1,), f32),
            pltpu.SMEM((1,), f32),
            pltpu.VMEM(routes.T.shape, jnp.int32),
            pltpu.VMEM(routes.T.shape, f32),
            pltpu.VMEM((model_width, head_dim), bf16),
            pltpu.VMEM((model_width, head_dim), bf16),
            pltpu.VMEM((model_width, head_dim), bf16),
            pltpu.VMEM((seq_rows, head_dim, head_dim), f32),
            pltpu.VMEM((head_dim, model_width), bf16),
            pltpu.VMEM((3 * model_width, hidden), bf16),
            pltpu.VMEM((seq_rows, head_dim), f32),
            pltpu.VMEM((seq_rows, head_dim), f32),
            pltpu.SemaphoreType.DMA((17 + model_width // hidden,)),
        ],
    )(
        parity,
        tokens,
        mixer_gain.reshape(1, model_width),
        write_weight.reshape(1, model_width),
        decay_weight.reshape(1, model_width),
        head_gain.reshape(1, head_dim),
        decay_rate,
        decay_bias,
        routes.T,
        route_weights.T,
        query_weight,
        key_weight,
        value_weight,
        state,
        out_weight,
        expert_gate[0],
        expert_up[0],
        expert_down[0],
    )
    gathered = lax.all_to_all(partials, "tp", 0, 0, tiled=True)
    next_state = pl.pallas_call(
        state_kernel,
        out_shape=jax.ShapeDtypeStruct((seq_rows, head_dim, head_dim), f32),
        in_specs=[vmem()] * 3 + [anywhere()],
        out_specs=anywhere(),
        scratch_shapes=[
            pltpu.VMEM((seq_rows, head_dim, head_dim), f32),
            pltpu.VMEM((seq_rows, head_dim, head_dim), f32),
            pltpu.SemaphoreType.DMA((4,)),
        ],
    )(in_vmem(key_unit), in_vmem(update), in_vmem(keep), state)
    other = lax.ppermute(packed, "tp", [(i, i ^ 1) for i in range(tp_count)])
    lanes = model_width // 128
    residual, expert_input, outgoing = pl.pallas_call(
        rows_kernel,
        out_shape=[
            pltpu.VMEM((seq_rows, model_width), bf16),
            pltpu.VMEM((seq_rows, model_width), bf16),
            jax.ShapeDtypeStruct((ep_count * lanes, 128), bf16),
        ],
        in_specs=[vmem()] * 4,
        out_specs=[vmem()] * 3,
        scratch_shapes=[pltpu.VMEM((ep_count * lanes, 128), f32)],
    )(
        in_vmem(gathered),
        in_vmem(tokens),
        in_vmem(channel_gain.reshape(1, model_width)),
        in_vmem(dispatch),
    )
    received = lax.all_to_all(outgoing.reshape(ep_count, lanes, 128), "ep", 0, 0, tiled=True)
    shared_act = (
        jax.nn.silu(jnp.dot(expert_input, shared_gate, preferred_element_type=f32))
        * jnp.dot(expert_input, shared_up, preferred_element_type=f32)
    ).astype(bf16)
    shared_partial = jnp.dot(shared_act, shared_down, preferred_element_type=f32).astype(bf16)
    blocks = pl.pallas_call(
        expert_kernel,
        out_shape=pltpu.VMEM((tp_count, ep_count + seq_rows, share_width), bf16),
        in_specs=[vmem()] * 4,
        out_specs=vmem(),
        scratch_shapes=[
            pltpu.VMEM((ep_count * lanes, 128), f32),
            pltpu.VMEM((ep_count, model_width), bf16),
        ],
    )(
        in_vmem(received.reshape(ep_count * lanes, 128)),
        in_vmem(packed),
        in_vmem(other),
        in_vmem(shared_partial),
    )
    parts = lax.all_to_all(blocks, "tp", 0, 0, tiled=True)
    quads = 2 * (share_width // 128)
    expert_share, shared_out = pl.pallas_call(
        share_kernel,
        out_shape=[
            pltpu.VMEM((ep_count * quads, 128), bf16),
            pltpu.VMEM((seq_rows, share_width), f32),
        ],
        in_specs=[vmem()],
        out_specs=[vmem()] * 2,
        scratch_shapes=[pltpu.VMEM((ep_count * quads, 128), f32)],
    )(in_vmem(parts))
    returned = lax.all_to_all(expert_share.reshape(ep_count, quads, 128), "ep", 0, 0, tiled=True)
    layer_out = pl.pallas_call(
        final_kernel,
        out_shape=jax.ShapeDtypeStruct((seq_rows, share_width), bf16),
        in_specs=[smem()] + [vmem()] * 4,
        out_specs=vmem(),
        scratch_shapes=[pltpu.VMEM((ep_count * quads, 128), f32)],
    )(
        tp_index.astype(jnp.int32).reshape(1),
        in_vmem(returned.reshape(ep_count * quads, 128)),
        in_vmem(combine),
        in_vmem(residual),
        in_vmem(shared_out),
    )
    return (layer_out, next_state.reshape(delta_state.shape))


def solution(mesh):
    return jax.shard_map(
        per_device,
        mesh=mesh,
        in_specs=(
            P("ep", None),
            P("ep", "tp", None, None),
            P(),
            P(None, "tp"),
            P(None, "tp"),
            P(None, "tp"),
            P(None, "tp"),
            P(None, "tp"),
            P("tp"),
            P("tp"),
            P(),
            P("tp", None),
            P(),
            P("ep", None),
            P("ep", None),
            P("ep", None, "tp"),
            P("ep", None, "tp"),
            P("ep", "tp", None),
            P(None, "tp"),
            P(None, "tp"),
            P("tp", None),
        ),
        out_specs=(P("ep", "tp"), P("ep", "tp", None, None)),
        check_vma=False,
    )
```

```python
import jax
import jax.numpy as jnp
from jax import lax
from jax.experimental import pallas as pl
from jax.experimental.pallas import tpu as pltpu
from jax.sharding import PartitionSpec as P

EPS = 1e-06
ROUTED_SCALE = 2.5


def rms_rows(values, gain_vec):
    mean_square = jnp.mean(values * values, axis=-1, keepdims=True)
    return values * lax.rsqrt(mean_square + EPS) * gain_vec


def unit_rows(raw):
    vals = raw.astype(jnp.bfloat16).astype(jnp.float32)
    return vals * lax.rsqrt(jnp.sum(vals * vals, axis=-1, keepdims=True) + EPS)


def columns_of(rows):
    pad = jnp.zeros((128 - rows.shape[0], rows.shape[1]), rows.dtype)
    return jnp.concatenate([rows, pad], axis=0).T


def mixer_kernel(
    tokens_hbm,
    gain_hbm,
    write_hbm,
    decay_hbm,
    head_gain_hbm,
    rate_hbm,
    bias_hbm,
    routes_hbm,
    weights_hbm,
    query_hbm,
    key_hbm,
    value_hbm,
    state_hbm,
    out_weight_hbm,
    gate_hbm,
    up_hbm,
    down_hbm,
    partial_hbm,
    key_unit_ref,
    update_ref,
    keep_ref,
    dispatch_ref,
    combine_ref,
    packed_ref,
    tokens_v,
    gain_v,
    write_v,
    decay_v,
    head_gain_v,
    rate_v,
    bias_v,
    routes_v,
    weights_v,
    query_v,
    key_v,
    value_v,
    state_v,
    out_weight_v,
    partial_v,
    found_k,
    found_q,
    sems,
):
    seq_rows = tokens_hbm.shape[0]
    width, hidden = gate_hbm.shape
    half = seq_rows // 2
    wide_block = 2 * hidden
    pairs = [
        (tokens_hbm, tokens_v),
        (gain_hbm, gain_v),
        (write_hbm, write_v),
        (decay_hbm, decay_v),
        (rate_hbm, rate_v),
        (bias_hbm, bias_v),
        (routes_hbm, routes_v),
        (weights_hbm, weights_v),
        (query_hbm, query_v),
        (key_hbm, key_v),
        (value_hbm, value_v),
        (state_hbm.at[pl.ds(0, half)], state_v.at[pl.ds(0, half)]),
        (
            state_hbm.at[pl.ds(half, seq_rows - half)],
            state_v.at[pl.ds(half, seq_rows - half)],
        ),
        (head_gain_hbm, head_gain_v),
        (out_weight_hbm, out_weight_v),
        (gate_hbm, packed_ref.at[pl.ds(0, width), pl.ds(0, hidden)]),
        (up_hbm, packed_ref.at[pl.ds(0, width), pl.ds(hidden, hidden)]),
    ] + [
        (
            down_hbm.at[:, pl.ds(j * wide_block, wide_block)],
            packed_ref.at[pl.ds(width + j * hidden, hidden)],
        )
        for j in range(width // wide_block)
    ]
    loads = [pltpu.make_async_copy(src, dst, sems.at[i]) for i, (src, dst) in enumerate(pairs)]
    for copy in loads:
        copy.start()
    for copy in loads[:8]:
        copy.wait()
    normed = rms_rows(tokens_v[...].astype(jnp.float32), gain_v[...]).astype(jnp.bfloat16)
    wide = normed.astype(jnp.float32)
    write_logit = jnp.sum(wide * write_v[...].astype(jnp.float32), axis=-1, keepdims=True)
    decay_logit = jnp.sum(wide * decay_v[...].astype(jnp.float32), axis=-1, keepdims=True)
    write_rate = 1.0 / (1.0 + jnp.exp(-write_logit))
    biased = decay_logit + bias_v[0]
    softplus = jnp.maximum(biased, 0.0) + jnp.log1p(jnp.exp(-jnp.abs(biased)))
    keep = jnp.exp(-rate_v[0] * softplus)
    routes = columns_of(routes_v[...].astype(jnp.float32))[:seq_rows].astype(jnp.int32)
    weights = columns_of(weights_v[...])[:seq_rows]
    scale = weights / jnp.sum(weights, axis=1, keepdims=True) * ROUTED_SCALE
    expert_iota = lax.broadcasted_iota(jnp.int32, (seq_rows, 128), 1)
    named = jnp.zeros((seq_rows, 128), jnp.float32)
    mix = jnp.zeros((seq_rows, 128), jnp.float32)
    for route in range(routes_hbm.shape[0]):
        hit = expert_iota == routes[:, route : route + 1]
        named = named + jnp.where(hit, 1.0, 0.0)
        mix = mix + jnp.where(hit, scale[:, route : route + 1], 0.0)
    row_a = lax.broadcasted_iota(jnp.int32, (seq_rows, seq_rows), 0)
    row_b = lax.broadcasted_iota(jnp.int32, (seq_rows, seq_rows), 1)
    below = jnp.where(row_b < row_a, 1.0, 0.0)
    earlier = jnp.dot(below, named, preferred_element_type=jnp.float32)
    slot = earlier.astype(jnp.int32)
    dispatch_ref[...] = jnp.where(slot == lax.axis_index("tp") % 2, named, 0.0).astype(jnp.bfloat16)
    combine_ref[0] = jnp.where(slot == 0, mix, 0.0)
    combine_ref[1] = jnp.where(slot == 1, mix, 0.0)
    loads[8].wait()
    query_raw = jnp.dot(normed, query_v[...], preferred_element_type=jnp.float32)
    loads[9].wait()
    key_raw = jnp.dot(normed, key_v[...], preferred_element_type=jnp.float32)
    loads[10].wait()
    value_raw = jnp.dot(normed, value_v[...], preferred_element_type=jnp.float32)
    query_unit = unit_rows(query_raw) * query_raw.shape[1] ** (-0.5)
    key_unit = unit_rows(key_raw)
    value_vec = value_raw.astype(jnp.bfloat16).astype(jnp.float32)
    key_cols = columns_of(key_unit)
    query_cols = columns_of(query_unit)
    for row in range(seq_rows):
        if row == 0:
            loads[11].wait()
        if row == half:
            loads[12].wait()
        state = state_v[row]
        found_k[row : row + 1, :] = jnp.sum(
            state * key_cols[:, row : row + 1], axis=0, keepdims=True
        )
        found_q[row : row + 1, :] = jnp.sum(
            state * query_cols[:, row : row + 1], axis=0, keepdims=True
        )
    loads[13].wait()
    correction = value_vec - keep * found_k[...]
    overlap = jnp.sum(key_unit * query_unit, axis=-1, keepdims=True)
    update = write_rate * correction
    readout = keep * found_q[...] + overlap * update
    head_out = rms_rows(readout, head_gain_v[...]).astype(jnp.bfloat16)
    loads[14].wait()
    partial = jnp.dot(head_out, out_weight_v[...], preferred_element_type=jnp.float32)
    partial = partial.astype(jnp.bfloat16)
    for copy_number in range(partial_v.shape[0]):
        partial_v[copy_number] = partial
    store = pltpu.make_async_copy(partial_v, partial_hbm, sems.at[0])
    store.start()
    key_unit_ref[...] = key_unit
    update_ref[...] = update
    keep_ref[...] = jnp.broadcast_to(keep, keep_ref.shape)
    for copy in loads[15:]:
        copy.wait()
    store.wait()


def rows_kernel(
    gathered_ref,
    tokens_ref,
    gain_ref,
    dispatch_ref,
    residual_ref,
    input_ref,
    rows_ref,
    wide_v,
):
    mixed = jnp.sum(gathered_ref[...].astype(jnp.float32), axis=0)
    mixed = mixed.astype(jnp.bfloat16).astype(jnp.float32)
    residual = (tokens_ref[...].astype(jnp.float32) + mixed).astype(jnp.bfloat16)
    inputs = rms_rows(residual.astype(jnp.float32), gain_ref[...]).astype(jnp.bfloat16)
    residual_ref[...] = residual
    input_ref[...] = inputs
    experts = dispatch_ref.shape[1]
    picked = lax.dot_general(
        dispatch_ref[...], inputs, (((0,), (0,)), ((), ())), preferred_element_type=jnp.float32
    )
    lanes = inputs.shape[1] // 128
    for lane in range(lanes):
        wide_v[pl.ds(lane, experts, stride=lanes), :] = picked[:, lane * 128 : (lane + 1) * 128]
    rows_ref[...] = wide_v[...].astype(jnp.bfloat16)


def expert_kernel(
    rows_ref,
    own_ref,
    other_ref,
    shared_ref,
    blocks_ref,
    wide_v,
    rows_v,
):
    lanes = 8
    experts = rows_ref.shape[0] // lanes
    width = lanes * 128
    wide_v[...] = rows_ref[...].astype(jnp.float32)
    for lane in range(lanes):
        rows_v[:, lane * 128 : (lane + 1) * 128] = wide_v[
            pl.ds(lane, experts, stride=lanes), :
        ].astype(jnp.bfloat16)
    rows = rows_v[...]
    acts = []
    for pack_ref in (own_ref, other_ref):
        both = jnp.dot(rows, pack_ref[:width], preferred_element_type=jnp.float32)
        gate, up = both[:, :128], both[:, 128:]
        acts.append((gate / (1.0 + jnp.exp(-gate)) * up).astype(jnp.bfloat16))
    act = jnp.concatenate(acts, axis=1)
    parts = blocks_ref.shape[0]
    share = width // parts
    for part in range(parts):
        at = width + part * 128
        down = jnp.concatenate([own_ref[at : at + 128], other_ref[at : at + 128]], axis=0)
        total = jnp.dot(act, down, preferred_element_type=jnp.float32)
        blocks_ref[part, :experts, :] = total.astype(jnp.bfloat16)
        blocks_ref[part, experts:, :] = shared_ref[:, part * share : (part + 1) * share]


def share_kernel(parts_ref, rows_ref, shared_ref, wide_v):
    share = parts_ref.shape[2]
    seq_rows = shared_ref.shape[0]
    experts = parts_ref.shape[1] - seq_rows
    quads = rows_ref.shape[0] // experts
    chunks = share // 128
    for slot in range(2):
        total = parts_ref[slot, :experts, :].astype(jnp.float32)
        total += parts_ref[slot + 2, :experts, :].astype(jnp.float32)
        for chunk in range(chunks):
            wide_v[pl.ds(slot * chunks + chunk, experts, stride=quads), :] = total[
                :, chunk * 128 : (chunk + 1) * 128
            ]
    rows_ref[...] = wide_v[...].astype(jnp.bfloat16)
    shared = jnp.sum(parts_ref[:, experts:, :].astype(jnp.float32), axis=0)
    shared_ref[...] = shared.astype(jnp.bfloat16).astype(jnp.float32)


def final_kernel(rows_ref, mix_ref, residual_ref, shared_ref, out_ref):
    seq_rows, share = out_ref.shape
    chunks = share // 128
    found = jnp.dot(mix_ref[...], rows_ref[...], preferred_element_type=jnp.float32)
    at = pl.multiple_of(lax.axis_index("tp") * share, share)
    base = residual_ref[:, pl.ds(at, share)].astype(jnp.float32) + shared_ref[...]
    for chunk in range(chunks):
        high = found[chunk * 32 : chunk * 32 + seq_rows]
        low = found[(chunks + chunk) * 32 : (chunks + chunk) * 32 + seq_rows]
        total = base[:, chunk * 128 : (chunk + 1) * 128] + (high + low)
        out_ref[:, chunk * 128 : (chunk + 1) * 128] = total.astype(jnp.bfloat16)


def state_kernel(
    key_unit_ref,
    update_ref,
    keep_ref,
    combine_ref,
    state_hbm,
    next_hbm,
    mix_ref,
    state_v,
    next_v,
    sems,
):
    seq_rows = key_unit_ref.shape[0]
    half = seq_rows // 2
    spans = [(0, half), (half, seq_rows - half)]
    loads = [
        pltpu.make_async_copy(
            state_hbm.at[pl.ds(at, size)], state_v.at[pl.ds(at, size)], sems.at[i]
        )
        for i, (at, size) in enumerate(spans)
    ]
    stores = [
        pltpu.make_async_copy(
            next_v.at[pl.ds(at, size)], next_hbm.at[pl.ds(at, size)], sems.at[2 + i]
        )
        for i, (at, size) in enumerate(spans)
    ]
    for copy in loads:
        copy.start()
    slots, _, experts = combine_ref.shape
    chunks = mix_ref.shape[0] // 64
    spread = slots * chunks * experts
    lane = lax.broadcasted_iota(jnp.int32, (experts, spread), 1)
    place = lax.broadcasted_iota(jnp.int32, (experts, spread), 0)
    expand = jnp.where(lane // (slots * chunks) == place, 1.0, 0.0).astype(jnp.bfloat16)
    member = lax.broadcasted_iota(jnp.int32, (seq_rows, spread), 1) % (slots * chunks)
    mix_ref[...] = jnp.zeros(mix_ref.shape, mix_ref.dtype)
    for slot in range(slots):
        full = combine_ref[slot]
        high = full.astype(jnp.bfloat16)
        low = (full - high.astype(jnp.float32)).astype(jnp.bfloat16)
        for part, term in enumerate((high, low)):
            grown = jnp.dot(term, expand, preferred_element_type=jnp.float32)
            for chunk in range(chunks):
                at = (part * chunks + chunk) * 32
                kept = jnp.where(member == slot * chunks + chunk, grown, 0.0)
                mix_ref[at : at + seq_rows, :] += kept.astype(jnp.bfloat16)
    key_cols = columns_of(key_unit_ref[...])
    for part, (at, size) in enumerate(spans):
        loads[part].wait()
        for row in range(at, at + size):
            next_v[row] = (
                keep_ref[row : row + 1, :] * state_v[row]
                + key_cols[:, row : row + 1] * update_ref[row : row + 1, :]
            )
        stores[part].start()
    for copy in stores:
        copy.wait()


def vmem():
    return pl.BlockSpec(memory_space=pltpu.VMEM)


def anywhere():
    return pl.BlockSpec(memory_space=pl.ANY)


def in_vmem(array):
    return pltpu.with_memory_space_constraint(array, pltpu.VMEM)


def per_device(
    tokens,
    delta_state,
    mixer_gain,
    query_weight,
    key_weight,
    value_weight,
    write_weight,
    decay_weight,
    decay_rate,
    decay_bias,
    head_gain,
    out_weight,
    channel_gain,
    routes,
    route_weights,
    expert_gate,
    expert_up,
    expert_down,
    shared_gate,
    shared_up,
    shared_down,
):
    seq_rows, model_width = tokens.shape
    head_dim = delta_state.shape[2]
    tp_count = lax.axis_size("tp")
    ep_count = lax.axis_size("ep")
    share_width = model_width // tp_count
    hidden = expert_gate.shape[2]
    quads = 2 * (share_width // 128)
    f32, bf16 = jnp.float32, jnp.bfloat16
    state = delta_state.reshape(seq_rows, head_dim, head_dim)
    small = pltpu.VMEM((seq_rows, head_dim), f32)
    partials, key_unit, update, keep, dispatch, combine, packed = pl.pallas_call(
        mixer_kernel,
        out_shape=[
            jax.ShapeDtypeStruct((tp_count, seq_rows, model_width), bf16),
            small,
            small,
            small,
            pltpu.VMEM((seq_rows, ep_count), bf16),
            pltpu.VMEM((2, seq_rows, ep_count), f32),
            pltpu.VMEM((3 * model_width // 2, 2 * hidden), bf16),
        ],
        in_specs=[anywhere()] * 17,
        out_specs=[anywhere()] + [vmem()] * 6,
        scratch_shapes=[
            pltpu.VMEM((seq_rows, model_width), bf16),
            pltpu.VMEM((1, model_width), f32),
            pltpu.VMEM((1, model_width), bf16),
            pltpu.VMEM((1, model_width), bf16),
            pltpu.VMEM((1, head_dim), f32),
            pltpu.SMEM((1,), f32),
            pltpu.SMEM((1,), f32),
            pltpu.VMEM(routes.T.shape, jnp.int32),
            pltpu.VMEM(routes.T.shape, f32),
            pltpu.VMEM((model_width, head_dim), bf16),
            pltpu.VMEM((model_width, head_dim), bf16),
            pltpu.VMEM((model_width, head_dim), bf16),
            pltpu.VMEM((seq_rows, head_dim, head_dim), f32),
            pltpu.VMEM((head_dim, model_width), bf16),
            pltpu.VMEM((tp_count, seq_rows, model_width), bf16),
            pltpu.VMEM((seq_rows, head_dim), f32),
            pltpu.VMEM((seq_rows, head_dim), f32),
            pltpu.SemaphoreType.DMA((17 + model_width // (2 * hidden),)),
        ],
    )(
        tokens,
        mixer_gain.reshape(1, model_width),
        write_weight.reshape(1, model_width),
        decay_weight.reshape(1, model_width),
        head_gain.reshape(1, head_dim),
        decay_rate,
        decay_bias,
        routes.T,
        route_weights.T,
        query_weight,
        key_weight,
        value_weight,
        state,
        out_weight,
        expert_gate[0],
        expert_up[0],
        expert_down[0],
    )
    gathered = lax.all_to_all(partials, "tp", 0, 0, tiled=True)
    next_state, mix = pl.pallas_call(
        state_kernel,
        out_shape=[
            jax.ShapeDtypeStruct((seq_rows, head_dim, head_dim), f32),
            pltpu.VMEM((64 * (share_width // 128), ep_count * quads), bf16),
        ],
        in_specs=[vmem()] * 4 + [anywhere()],
        out_specs=[anywhere(), vmem()],
        scratch_shapes=[
            pltpu.VMEM((seq_rows, head_dim, head_dim), f32),
            pltpu.VMEM((seq_rows, head_dim, head_dim), f32),
            pltpu.SemaphoreType.DMA((4,)),
        ],
    )(
        in_vmem(key_unit), in_vmem(update), in_vmem(keep), in_vmem(combine), state
    )
    other = lax.ppermute(packed, "tp", [(i, i ^ 1) for i in range(tp_count)])
    lanes = model_width // 128
    residual, expert_input, outgoing = pl.pallas_call(
        rows_kernel,
        out_shape=[
            pltpu.VMEM((seq_rows, model_width), bf16),
            pltpu.VMEM((seq_rows, model_width), bf16),
            jax.ShapeDtypeStruct((ep_count * lanes, 128), bf16),
        ],
        in_specs=[vmem()] * 4,
        out_specs=[vmem()] * 3,
        scratch_shapes=[pltpu.VMEM((ep_count * lanes, 128), f32)],
    )(
        in_vmem(gathered),
        in_vmem(tokens),
        in_vmem(channel_gain.reshape(1, model_width)),
        in_vmem(dispatch),
    )
    received = lax.all_to_all(outgoing.reshape(ep_count, lanes, 128), "ep", 0, 0, tiled=True)
    shared_act = (
        jax.nn.silu(jnp.dot(expert_input, shared_gate, preferred_element_type=f32))
        * jnp.dot(expert_input, shared_up, preferred_element_type=f32)
    ).astype(bf16)
    shared_partial = jnp.dot(shared_act, shared_down, preferred_element_type=f32).astype(bf16)
    blocks = pl.pallas_call(
        expert_kernel,
        out_shape=pltpu.VMEM((tp_count, ep_count + seq_rows, share_width), bf16),
        in_specs=[vmem()] * 4,
        out_specs=vmem(),
        scratch_shapes=[
            pltpu.VMEM((ep_count * lanes, 128), f32),
            pltpu.VMEM((ep_count, model_width), bf16),
        ],
    )(
        in_vmem(received.reshape(ep_count * lanes, 128)),
        in_vmem(packed),
        in_vmem(other),
        in_vmem(shared_partial),
    )
    parts = lax.all_to_all(blocks, "tp", 0, 0, tiled=True)
    expert_share, shared_out = pl.pallas_call(
        share_kernel,
        out_shape=[
            pltpu.VMEM((ep_count * quads, 128), bf16),
            pltpu.VMEM((seq_rows, share_width), f32),
        ],
        in_specs=[vmem()],
        out_specs=[vmem()] * 2,
        scratch_shapes=[pltpu.VMEM((ep_count * quads, 128), f32)],
    )(in_vmem(parts))
    returned = lax.all_to_all(expert_share.reshape(ep_count, quads, 128), "ep", 0, 0, tiled=True)
    layer_out = pl.pallas_call(
        final_kernel,
        out_shape=jax.ShapeDtypeStruct((seq_rows, share_width), bf16),
        in_specs=[vmem()] * 4,
        out_specs=vmem(),
    )(
        in_vmem(returned.reshape(ep_count * quads, 128)),
        in_vmem(mix),
        in_vmem(residual),
        in_vmem(shared_out),
    )
    return (layer_out, next_state.reshape(delta_state.shape))


def solution(mesh):
    return jax.shard_map(
        per_device,
        mesh=mesh,
        in_specs=(
            P("ep", None),
            P("ep", "tp", None, None),
            P(),
            P(None, "tp"),
            P(None, "tp"),
            P(None, "tp"),
            P(None, "tp"),
            P(None, "tp"),
            P("tp"),
            P("tp"),
            P(),
            P("tp", None),
            P(),
            P("ep", None),
            P("ep", None),
            P("ep", None, "tp"),
            P("ep", None, "tp"),
            P("ep", "tp", None),
            P(None, "tp"),
            P(None, "tp"),
            P("tp", None),
        ),
        out_specs=(P("ep", "tp"), P("ep", "tp", None, None)),
        check_vma=False,
    )
```

```python
import jax
import jax.numpy as jnp
from jax import lax
from jax.experimental import pallas as pl
from jax.experimental.pallas import tpu as pltpu
from jax.sharding import PartitionSpec as P

EPS = 1e-06
ROUTED_SCALE = 2.5


def rms_rows(values, gain_vec):
    mean_square = jnp.mean(values * values, axis=-1, keepdims=True)
    return values * lax.rsqrt(mean_square + EPS) * gain_vec


def unit_rows(raw):
    vals = raw.astype(jnp.bfloat16).astype(jnp.float32)
    return vals * lax.rsqrt(jnp.sum(vals * vals, axis=-1, keepdims=True) + EPS)


def columns_of(rows):
    pad = jnp.zeros((128 - rows.shape[0], rows.shape[1]), rows.dtype)
    return jnp.concatenate([rows, pad], axis=0).T


def mixer_kernel(
    tokens_hbm,
    gain_hbm,
    write_hbm,
    decay_hbm,
    head_gain_hbm,
    rate_hbm,
    bias_hbm,
    routes_hbm,
    weights_hbm,
    query_hbm,
    key_hbm,
    value_hbm,
    state_hbm,
    out_weight_hbm,
    gate_hbm,
    up_hbm,
    down_hbm,
    partial_hbm,
    next_hbm,
    dispatch_ref,
    mix_ref,
    packed_ref,
    tokens_v,
    gain_v,
    write_v,
    decay_v,
    head_gain_v,
    rate_v,
    bias_v,
    routes_v,
    weights_v,
    query_v,
    key_v,
    value_v,
    state_v,
    next_v,
    out_weight_v,
    partial_v,
    found_k,
    found_q,
    sems,
):
    seq_rows = tokens_hbm.shape[0]
    width, hidden = gate_hbm.shape
    half = seq_rows // 2
    wide_block = 2 * hidden
    pairs = [
        (tokens_hbm, tokens_v),
        (gain_hbm, gain_v),
        (write_hbm, write_v),
        (decay_hbm, decay_v),
        (rate_hbm, rate_v),
        (bias_hbm, bias_v),
        (routes_hbm, routes_v),
        (weights_hbm, weights_v),
        (query_hbm, query_v),
        (key_hbm, key_v),
        (value_hbm, value_v),
        (state_hbm.at[pl.ds(0, half)], state_v.at[pl.ds(0, half)]),
        (
            state_hbm.at[pl.ds(half, seq_rows - half)],
            state_v.at[pl.ds(half, seq_rows - half)],
        ),
        (head_gain_hbm, head_gain_v),
        (out_weight_hbm, out_weight_v),
        (gate_hbm, packed_ref.at[pl.ds(0, width), pl.ds(0, hidden)]),
        (up_hbm, packed_ref.at[pl.ds(0, width), pl.ds(hidden, hidden)]),
    ] + [
        (
            down_hbm.at[:, pl.ds(j * wide_block, wide_block)],
            packed_ref.at[pl.ds(width + j * hidden, hidden)],
        )
        for j in range(width // wide_block)
    ]
    loads = [pltpu.make_async_copy(src, dst, sems.at[i]) for i, (src, dst) in enumerate(pairs)]
    for copy in loads:
        copy.start()
    for copy in loads[:8]:
        copy.wait()
    normed = rms_rows(tokens_v[...].astype(jnp.float32), gain_v[...]).astype(jnp.bfloat16)
    wide = normed.astype(jnp.float32)
    write_logit = jnp.sum(wide * write_v[...].astype(jnp.float32), axis=-1, keepdims=True)
    decay_logit = jnp.sum(wide * decay_v[...].astype(jnp.float32), axis=-1, keepdims=True)
    write_rate = 1.0 / (1.0 + jnp.exp(-write_logit))
    biased = decay_logit + bias_v[0]
    softplus = jnp.maximum(biased, 0.0) + jnp.log1p(jnp.exp(-jnp.abs(biased)))
    keep = jnp.exp(-rate_v[0] * softplus)
    routes = columns_of(routes_v[...].astype(jnp.float32))[:seq_rows].astype(jnp.int32)
    weights = columns_of(weights_v[...])[:seq_rows]
    scale = weights / jnp.sum(weights, axis=1, keepdims=True) * ROUTED_SCALE
    expert_iota = lax.broadcasted_iota(jnp.int32, (seq_rows, 128), 1)
    named = jnp.zeros((seq_rows, 128), jnp.float32)
    mix = jnp.zeros((seq_rows, 128), jnp.float32)
    for route in range(routes_hbm.shape[0]):
        hit = expert_iota == routes[:, route : route + 1]
        named = named + jnp.where(hit, 1.0, 0.0)
        mix = mix + jnp.where(hit, scale[:, route : route + 1], 0.0)
    row_a = lax.broadcasted_iota(jnp.int32, (seq_rows, seq_rows), 0)
    row_b = lax.broadcasted_iota(jnp.int32, (seq_rows, seq_rows), 1)
    below = jnp.where(row_b < row_a, 1.0, 0.0)
    earlier = jnp.dot(below, named, preferred_element_type=jnp.float32)
    chosen = earlier.astype(jnp.int32)
    dispatch_ref[...] = jnp.where(chosen == lax.axis_index("tp") % 2, named, 0.0).astype(jnp.bfloat16)
    loads[8].wait()
    query_raw = jnp.dot(normed, query_v[...], preferred_element_type=jnp.float32)
    loads[9].wait()
    key_raw = jnp.dot(normed, key_v[...], preferred_element_type=jnp.float32)
    loads[10].wait()
    value_raw = jnp.dot(normed, value_v[...], preferred_element_type=jnp.float32)
    query_unit = unit_rows(query_raw) * query_raw.shape[1] ** (-0.5)
    key_unit = unit_rows(key_raw)
    value_vec = value_raw.astype(jnp.bfloat16).astype(jnp.float32)
    key_cols = columns_of(key_unit)
    query_cols = columns_of(query_unit)
    for row in range(seq_rows):
        if row == 0:
            loads[11].wait()
        if row == half:
            loads[12].wait()
        state = state_v[row]
        found_k[row : row + 1, :] = jnp.sum(
            state * key_cols[:, row : row + 1], axis=0, keepdims=True
        )
        found_q[row : row + 1, :] = jnp.sum(
            state * query_cols[:, row : row + 1], axis=0, keepdims=True
        )
    loads[13].wait()
    correction = value_vec - keep * found_k[...]
    overlap = jnp.sum(key_unit * query_unit, axis=-1, keepdims=True)
    update = write_rate * correction
    readout = keep * found_q[...] + overlap * update
    head_out = rms_rows(readout, head_gain_v[...]).astype(jnp.bfloat16)
    loads[14].wait()
    partial = jnp.dot(head_out, out_weight_v[...], preferred_element_type=jnp.float32)
    partial = partial.astype(jnp.bfloat16)
    for copy_number in range(partial_v.shape[0]):
        partial_v[copy_number] = partial
    store = pltpu.make_async_copy(partial_v, partial_hbm, sems.at[0])
    store.start()
    keep_rows = jnp.broadcast_to(keep, update.shape)
    stores = [store]
    step = 3
    for at in range(0, seq_rows, step):
        for row in range(at, at + step):
            next_v[row] = (
                keep_rows[row : row + 1, :] * state_v[row]
                + key_cols[:, row : row + 1] * update[row : row + 1, :]
            )
        store = pltpu.make_async_copy(
            next_v.at[pl.ds(at, step)], next_hbm.at[pl.ds(at, step)], sems.at[1 + at // step]
        )
        store.start()
        stores.append(store)
    slots, experts = 2, dispatch_ref.shape[1]
    chunks = mix_ref.shape[0] // 64
    spread = slots * chunks * experts
    lane = lax.broadcasted_iota(jnp.int32, (experts, spread), 1)
    place = lax.broadcasted_iota(jnp.int32, (experts, spread), 0)
    expand = jnp.where(lane // (slots * chunks) == place, 1.0, 0.0).astype(jnp.bfloat16)
    member = lax.broadcasted_iota(jnp.int32, (seq_rows, spread), 1) % (slots * chunks)
    mix_ref[...] = jnp.zeros(mix_ref.shape, mix_ref.dtype)
    for slot in range(slots):
        full = jnp.where(chosen == slot, mix, 0.0)
        high = full.astype(jnp.bfloat16)
        low = (full - high.astype(jnp.float32)).astype(jnp.bfloat16)
        for part, term in enumerate((high, low)):
            grown = jnp.dot(term, expand, preferred_element_type=jnp.float32)
            for chunk in range(chunks):
                at = (part * chunks + chunk) * 32
                kept = jnp.where(member == slot * chunks + chunk, grown, 0.0)
                mix_ref[at : at + seq_rows, :] += kept.astype(jnp.bfloat16)
    for copy in loads[15:]:
        copy.wait()
    for copy in stores:
        copy.wait()


def rows_kernel(
    gathered_ref,
    tokens_ref,
    gain_ref,
    dispatch_ref,
    residual_ref,
    input_ref,
    rows_ref,
    wide_v,
):
    mixed = jnp.sum(gathered_ref[...].astype(jnp.float32), axis=0)
    mixed = mixed.astype(jnp.bfloat16).astype(jnp.float32)
    residual = (tokens_ref[...].astype(jnp.float32) + mixed).astype(jnp.bfloat16)
    inputs = rms_rows(residual.astype(jnp.float32), gain_ref[...]).astype(jnp.bfloat16)
    residual_ref[...] = residual
    input_ref[...] = inputs
    experts = dispatch_ref.shape[1]
    picked = lax.dot_general(
        dispatch_ref[...], inputs, (((0,), (0,)), ((), ())), preferred_element_type=jnp.float32
    )
    lanes = inputs.shape[1] // 128
    for lane in range(lanes):
        wide_v[pl.ds(lane, experts, stride=lanes), :] = picked[:, lane * 128 : (lane + 1) * 128]
    rows_ref[...] = wide_v[...].astype(jnp.bfloat16)


def expert_kernel(
    rows_ref,
    own_ref,
    other_ref,
    shared_ref,
    blocks_ref,
    wide_v,
    rows_v,
):
    lanes = 8
    experts = rows_ref.shape[0] // lanes
    width = lanes * 128
    wide_v[...] = rows_ref[...].astype(jnp.float32)
    for lane in range(lanes):
        rows_v[:, lane * 128 : (lane + 1) * 128] = wide_v[
            pl.ds(lane, experts, stride=lanes), :
        ].astype(jnp.bfloat16)
    rows = rows_v[...]
    acts = []
    for pack_ref in (own_ref, other_ref):
        both = jnp.dot(rows, pack_ref[:width], preferred_element_type=jnp.float32)
        gate, up = both[:, :128], both[:, 128:]
        acts.append((gate / (1.0 + jnp.exp(-gate)) * up).astype(jnp.bfloat16))
    act = jnp.concatenate(acts, axis=1)
    parts = blocks_ref.shape[0]
    share = width // parts
    for part in range(parts):
        at = width + part * 128
        down = jnp.concatenate([own_ref[at : at + 128], other_ref[at : at + 128]], axis=0)
        total = jnp.dot(act, down, preferred_element_type=jnp.float32)
        blocks_ref[part, :experts, :] = total.astype(jnp.bfloat16)
        blocks_ref[part, experts:, :] = shared_ref[:, part * share : (part + 1) * share]


def share_kernel(parts_ref, rows_ref, shared_ref, wide_v):
    share = parts_ref.shape[2]
    seq_rows = shared_ref.shape[0]
    experts = parts_ref.shape[1] - seq_rows
    quads = rows_ref.shape[0] // experts
    chunks = share // 128
    for slot in range(2):
        total = parts_ref[slot, :experts, :].astype(jnp.float32)
        total += parts_ref[slot + 2, :experts, :].astype(jnp.float32)
        for chunk in range(chunks):
            wide_v[pl.ds(slot * chunks + chunk, experts, stride=quads), :] = total[
                :, chunk * 128 : (chunk + 1) * 128
            ]
    rows_ref[...] = wide_v[...].astype(jnp.bfloat16)
    shared = jnp.sum(parts_ref[:, experts:, :].astype(jnp.float32), axis=0)
    shared_ref[...] = shared.astype(jnp.bfloat16).astype(jnp.float32)


def final_kernel(rows_ref, mix_ref, residual_ref, shared_ref, out_ref):
    seq_rows, share = out_ref.shape
    chunks = share // 128
    found = jnp.dot(mix_ref[...], rows_ref[...], preferred_element_type=jnp.float32)
    at = pl.multiple_of(lax.axis_index("tp") * share, share)
    base = residual_ref[:, pl.ds(at, share)].astype(jnp.float32) + shared_ref[...]
    for chunk in range(chunks):
        high = found[chunk * 32 : chunk * 32 + seq_rows]
        low = found[(chunks + chunk) * 32 : (chunks + chunk) * 32 + seq_rows]
        total = base[:, chunk * 128 : (chunk + 1) * 128] + (high + low)
        out_ref[:, chunk * 128 : (chunk + 1) * 128] = total.astype(jnp.bfloat16)


def vmem():
    return pl.BlockSpec(memory_space=pltpu.VMEM)


def anywhere():
    return pl.BlockSpec(memory_space=pl.ANY)


def in_vmem(array):
    return pltpu.with_memory_space_constraint(array, pltpu.VMEM)


def per_device(
    tokens,
    delta_state,
    mixer_gain,
    query_weight,
    key_weight,
    value_weight,
    write_weight,
    decay_weight,
    decay_rate,
    decay_bias,
    head_gain,
    out_weight,
    channel_gain,
    routes,
    route_weights,
    expert_gate,
    expert_up,
    expert_down,
    shared_gate,
    shared_up,
    shared_down,
):
    seq_rows, model_width = tokens.shape
    head_dim = delta_state.shape[2]
    tp_count = lax.axis_size("tp")
    ep_count = lax.axis_size("ep")
    share_width = model_width // tp_count
    hidden = expert_gate.shape[2]
    quads = 2 * (share_width // 128)
    f32, bf16 = jnp.float32, jnp.bfloat16
    state = delta_state.reshape(seq_rows, head_dim, head_dim)
    partials, next_state, dispatch, mix, packed = pl.pallas_call(
        mixer_kernel,
        out_shape=[
            jax.ShapeDtypeStruct((tp_count, seq_rows, model_width), bf16),
            jax.ShapeDtypeStruct(state.shape, f32),
            pltpu.VMEM((seq_rows, ep_count), bf16),
            pltpu.VMEM((64 * (share_width // 128), ep_count * quads), bf16),
            pltpu.VMEM((3 * model_width // 2, 2 * hidden), bf16),
        ],
        in_specs=[anywhere()] * 17,
        out_specs=[anywhere()] * 2 + [vmem()] * 3,
        scratch_shapes=[
            pltpu.VMEM((seq_rows, model_width), bf16),
            pltpu.VMEM((1, model_width), f32),
            pltpu.VMEM((1, model_width), bf16),
            pltpu.VMEM((1, model_width), bf16),
            pltpu.VMEM((1, head_dim), f32),
            pltpu.SMEM((1,), f32),
            pltpu.SMEM((1,), f32),
            pltpu.VMEM(routes.T.shape, jnp.int32),
            pltpu.VMEM(routes.T.shape, f32),
            pltpu.VMEM((model_width, head_dim), bf16),
            pltpu.VMEM((model_width, head_dim), bf16),
            pltpu.VMEM((model_width, head_dim), bf16),
            pltpu.VMEM((seq_rows, head_dim, head_dim), f32),
            pltpu.VMEM((seq_rows, head_dim, head_dim), f32),
            pltpu.VMEM((head_dim, model_width), bf16),
            pltpu.VMEM((tp_count, seq_rows, model_width), bf16),
            pltpu.VMEM((seq_rows, head_dim), f32),
            pltpu.VMEM((seq_rows, head_dim), f32),
            pltpu.SemaphoreType.DMA((17 + model_width // (2 * hidden),)),
        ],
    )(
        tokens,
        mixer_gain.reshape(1, model_width),
        write_weight.reshape(1, model_width),
        decay_weight.reshape(1, model_width),
        head_gain.reshape(1, head_dim),
        decay_rate,
        decay_bias,
        routes.T,
        route_weights.T,
        query_weight,
        key_weight,
        value_weight,
        state,
        out_weight,
        expert_gate[0],
        expert_up[0],
        expert_down[0],
    )
    gathered = lax.all_to_all(partials, "tp", 0, 0, tiled=True)
    other = lax.ppermute(packed, "tp", [(i, i ^ 1) for i in range(tp_count)])
    lanes = model_width // 128
    residual, expert_input, outgoing = pl.pallas_call(
        rows_kernel,
        out_shape=[
            pltpu.VMEM((seq_rows, model_width), bf16),
            pltpu.VMEM((seq_rows, model_width), bf16),
            pltpu.VMEM((ep_count * lanes, 128), bf16),
        ],
        in_specs=[vmem()] * 4,
        out_specs=[vmem()] * 3,
        scratch_shapes=[pltpu.VMEM((ep_count * lanes, 128), f32)],
    )(
        in_vmem(gathered),
        in_vmem(tokens),
        in_vmem(channel_gain.reshape(1, model_width)),
        in_vmem(dispatch),
    )
    shared_act = (
        jax.nn.silu(jnp.dot(expert_input, shared_gate, preferred_element_type=f32))
        * jnp.dot(expert_input, shared_up, preferred_element_type=f32)
    ).astype(bf16)
    shared_partial = jnp.dot(shared_act, shared_down, preferred_element_type=f32).astype(bf16)
    outgoing, shared_partial = lax.optimization_barrier((outgoing, shared_partial))
    received = lax.all_to_all(outgoing.reshape(ep_count, lanes, 128), "ep", 0, 0, tiled=True)
    blocks = pl.pallas_call(
        expert_kernel,
        out_shape=pltpu.VMEM((tp_count, ep_count + seq_rows, share_width), bf16),
        in_specs=[vmem()] * 4,
        out_specs=vmem(),
        scratch_shapes=[
            pltpu.VMEM((ep_count * lanes, 128), f32),
            pltpu.VMEM((ep_count, model_width), bf16),
        ],
    )(
        in_vmem(received.reshape(ep_count * lanes, 128)),
        in_vmem(packed),
        in_vmem(other),
        in_vmem(shared_partial),
    )
    parts = lax.all_to_all(blocks, "tp", 0, 0, tiled=True)
    expert_share, shared_out = pl.pallas_call(
        share_kernel,
        out_shape=[
            pltpu.VMEM((ep_count * quads, 128), bf16),
            pltpu.VMEM((seq_rows, share_width), f32),
        ],
        in_specs=[vmem()],
        out_specs=[vmem()] * 2,
        scratch_shapes=[pltpu.VMEM((ep_count * quads, 128), f32)],
    )(in_vmem(parts))
    returned = lax.all_to_all(expert_share.reshape(ep_count, quads, 128), "ep", 0, 0, tiled=True)
    layer_out = pl.pallas_call(
        final_kernel,
        out_shape=jax.ShapeDtypeStruct((seq_rows, share_width), bf16),
        in_specs=[vmem()] * 4,
        out_specs=vmem(),
    )(
        in_vmem(returned.reshape(ep_count * quads, 128)),
        in_vmem(mix),
        in_vmem(residual),
        in_vmem(shared_out),
    )
    return (layer_out, next_state.reshape(delta_state.shape))


def solution(mesh):
    return jax.shard_map(
        per_device,
        mesh=mesh,
        in_specs=(
            P("ep", None),
            P("ep", "tp", None, None),
            P(),
            P(None, "tp"),
            P(None, "tp"),
            P(None, "tp"),
            P(None, "tp"),
            P(None, "tp"),
            P("tp"),
            P("tp"),
            P(),
            P("tp", None),
            P(),
            P("ep", None),
            P("ep", None),
            P("ep", None, "tp"),
            P("ep", None, "tp"),
            P("ep", "tp", None),
            P(None, "tp"),
            P(None, "tp"),
            P("tp", None),
        ),
        out_specs=(P("ep", "tp"), P("ep", "tp", None, None)),
        check_vma=False,
    )
```

```python
import jax
import jax.numpy as jnp
from jax import lax
from jax.experimental import pallas as pl
from jax.experimental.pallas import tpu as pltpu
from jax.sharding import PartitionSpec as P

EPS = 1e-06
ROUTED_SCALE = 2.5


def rms_rows(values, gain_vec):
    mean_square = jnp.mean(values * values, axis=-1, keepdims=True)
    return values * lax.rsqrt(mean_square + EPS) * gain_vec


def unit_rows(raw):
    vals = raw.astype(jnp.bfloat16).astype(jnp.float32)
    return vals * lax.rsqrt(jnp.sum(vals * vals, axis=-1, keepdims=True) + EPS)


def columns_of(rows):
    pad = jnp.zeros((128 - rows.shape[0], rows.shape[1]), rows.dtype)
    return jnp.concatenate([rows, pad], axis=0).T


def earlier_rows(named):
    seq_rows = named.shape[0]
    row_a = lax.broadcasted_iota(jnp.int32, (seq_rows, seq_rows), 0)
    row_b = lax.broadcasted_iota(jnp.int32, (seq_rows, seq_rows), 1)
    below = jnp.where(row_b < row_a, 1.0, 0.0)
    return jnp.dot(below, named, preferred_element_type=jnp.float32).astype(jnp.int32)


def picked_rows(routes, core, slot):
    seq_rows, top_k = routes.shape
    experts = 2 * lax.broadcasted_iota(jnp.int32, (seq_rows, 64), 1) + core
    named = jnp.zeros((seq_rows, 64), jnp.float32)
    for route in range(top_k):
        named = named + jnp.where(experts == routes[:, route : route + 1], 1.0, 0.0)
    return jnp.where(earlier_rows(named) == slot, named, 0.0).astype(jnp.bfloat16)


def mixer_kernel(
    tokens_hbm,
    gain_hbm,
    write_hbm,
    decay_hbm,
    head_gain_hbm,
    rate_hbm,
    bias_hbm,
    routes_hbm,
    weights_hbm,
    query_hbm,
    key_hbm,
    value_hbm,
    state_hbm,
    out_weight_hbm,
    gate_hbm,
    up_hbm,
    down_hbm,
    partial_hbm,
    next_hbm,
    mix_ref,
    packed_ref,
    tokens_v,
    gain_v,
    write_v,
    decay_v,
    head_gain_v,
    rate_v,
    bias_v,
    routes_v,
    weights_v,
    query_v,
    key_v,
    value_v,
    state_v,
    next_v,
    out_weight_v,
    partial_v,
    plain_v,
    mixed_v,
    found_k,
    found_q,
    sems,
):
    seq_rows = tokens_hbm.shape[0]
    core = lax.axis_index("ep") % 2
    tp_index = lax.axis_index("tp")
    width, hidden = gate_hbm.shape
    half = seq_rows // 2
    wide_block = 2 * hidden
    pairs = [
        (tokens_hbm, tokens_v),
        (gain_hbm, gain_v),
        (write_hbm, write_v),
        (decay_hbm, decay_v),
        (rate_hbm, rate_v),
        (bias_hbm, bias_v),
        (routes_hbm, routes_v),
        (weights_hbm, weights_v),
        (query_hbm, query_v),
        (key_hbm, key_v),
        (value_hbm, value_v),
        (state_hbm.at[pl.ds(0, half)], state_v.at[pl.ds(0, half)]),
        (
            state_hbm.at[pl.ds(half, seq_rows - half)],
            state_v.at[pl.ds(half, seq_rows - half)],
        ),
        (head_gain_hbm, head_gain_v),
        (out_weight_hbm, out_weight_v),
        (gate_hbm, packed_ref.at[pl.ds(0, width), pl.ds(0, hidden)]),
        (up_hbm, packed_ref.at[pl.ds(0, width), pl.ds(hidden, hidden)]),
    ] + [
        (
            down_hbm.at[:, pl.ds(j * wide_block, wide_block)],
            packed_ref.at[pl.ds(width + j * hidden, hidden)],
        )
        for j in range(width // wide_block)
    ]
    loads = [pltpu.make_async_copy(src, dst, sems.at[i]) for i, (src, dst) in enumerate(pairs)]
    for copy in loads:
        copy.start()
    for copy in loads[:8]:
        copy.wait()
    normed = rms_rows(tokens_v[...].astype(jnp.float32), gain_v[...]).astype(jnp.bfloat16)
    wide = normed.astype(jnp.float32)
    write_logit = jnp.sum(wide * write_v[...].astype(jnp.float32), axis=-1, keepdims=True)
    decay_logit = jnp.sum(wide * decay_v[...].astype(jnp.float32), axis=-1, keepdims=True)
    write_rate = 1.0 / (1.0 + jnp.exp(-write_logit))
    biased = decay_logit + bias_v[0]
    softplus = jnp.maximum(biased, 0.0) + jnp.log1p(jnp.exp(-jnp.abs(biased)))
    keep = jnp.exp(-rate_v[0] * softplus)
    routes = columns_of(routes_v[...].astype(jnp.float32))[:seq_rows].astype(jnp.int32)
    weights = columns_of(weights_v[...])[:seq_rows]
    scale = weights / jnp.sum(weights, axis=1, keepdims=True) * ROUTED_SCALE
    expert_iota = lax.broadcasted_iota(jnp.int32, (seq_rows, 128), 1)
    named = jnp.zeros((seq_rows, 128), jnp.float32)
    mix = jnp.zeros((seq_rows, 128), jnp.float32)
    for route in range(routes_hbm.shape[0]):
        hit = expert_iota == routes[:, route : route + 1]
        named = named + jnp.where(hit, 1.0, 0.0)
        mix = mix + jnp.where(hit, scale[:, route : route + 1], 0.0)
    chosen = earlier_rows(named)
    loads[8].wait()
    query_raw = jnp.dot(normed, query_v[...], preferred_element_type=jnp.float32)
    loads[9].wait()
    key_raw = jnp.dot(normed, key_v[...], preferred_element_type=jnp.float32)
    loads[10].wait()
    value_raw = jnp.dot(normed, value_v[...], preferred_element_type=jnp.float32)
    query_unit = unit_rows(query_raw) * query_raw.shape[1] ** (-0.5)
    key_unit = unit_rows(key_raw)
    value_vec = value_raw.astype(jnp.bfloat16).astype(jnp.float32)
    key_cols = columns_of(key_unit)
    query_cols = columns_of(query_unit)
    for row in range(seq_rows):
        if row == 0:
            loads[11].wait()
        if row == half:
            loads[12].wait()
        state = state_v[row]
        found_k[row : row + 1, :] = jnp.sum(
            state * key_cols[:, row : row + 1], axis=0, keepdims=True
        )
        found_q[row : row + 1, :] = jnp.sum(
            state * query_cols[:, row : row + 1], axis=0, keepdims=True
        )
    loads[13].wait()
    correction = value_vec - keep * found_k[...]
    overlap = jnp.sum(key_unit * query_unit, axis=-1, keepdims=True)
    update = write_rate * correction
    readout = keep * found_q[...] + overlap * update
    head_out = rms_rows(readout, head_gain_v[...]).astype(jnp.bfloat16)
    loads[14].wait()
    partial = jnp.dot(head_out, out_weight_v[...], preferred_element_type=jnp.float32)
    partial = partial.astype(jnp.bfloat16).astype(jnp.float32)
    mixed = partial + jnp.where(tp_index == 0, tokens_v[...].astype(jnp.float32), 0.0)
    lanes = width // 128
    top_k = routes_hbm.shape[0]
    for lane in range(lanes):
        part = slice(lane * 128, (lane + 1) * 128)
        plain_v[pl.ds(lane, seq_rows, stride=lanes), :] = partial[:, part]
        mixed_v[pl.ds(lane, seq_rows, stride=lanes), :] = mixed[:, part]
    plain_v[seq_rows * lanes :, :] = jnp.zeros((8, 128), jnp.float32)
    mixed_v[seq_rows * lanes :, :] = jnp.zeros((8, 128), jnp.float32)
    names = slice(seq_rows * lanes, seq_rows * lanes + top_k)
    plain_v[names, :seq_rows] = routes_v[...].astype(jnp.float32)
    mixed_v[names, :seq_rows] = routes_v[...].astype(jnp.float32)
    plain = plain_v[...].astype(jnp.bfloat16)
    mixed = mixed_v[...].astype(jnp.bfloat16)
    group = partial_v.shape[0] // 2
    for copy_number in range(partial_v.shape[0]):
        partial_v[copy_number] = jnp.where(core == copy_number // group, plain, mixed)
    store = pltpu.make_async_copy(partial_v, partial_hbm, sems.at[0])
    store.start()
    keep_rows = jnp.broadcast_to(keep, update.shape)
    stores = [store]
    step = 3
    for at in range(0, seq_rows, step):
        for row in range(at, at + step):
            next_v[row] = (
                keep_rows[row : row + 1, :] * state_v[row]
                + key_cols[:, row : row + 1] * update[row : row + 1, :]
            )
        store = pltpu.make_async_copy(
            next_v.at[pl.ds(at, step)], next_hbm.at[pl.ds(at, step)], sems.at[1 + at // step]
        )
        store.start()
        stores.append(store)
    slots, experts = 2, 128
    chunks = mix_ref.shape[0] // 64
    spread = slots * chunks * experts
    lane = lax.broadcasted_iota(jnp.int32, (experts, spread), 1)
    place = lax.broadcasted_iota(jnp.int32, (experts, spread), 0)
    expand = jnp.where(lane // (slots * chunks) == place, 1.0, 0.0).astype(jnp.bfloat16)
    member = lax.broadcasted_iota(jnp.int32, (seq_rows, spread), 1) % (slots * chunks)
    mix_ref[...] = jnp.zeros(mix_ref.shape, mix_ref.dtype)
    for slot in range(slots):
        full = jnp.where(chosen == slot, mix, 0.0)
        high = full.astype(jnp.bfloat16)
        low = (full - high.astype(jnp.float32)).astype(jnp.bfloat16)
        for part, term in enumerate((high, low)):
            grown = jnp.dot(term, expand, preferred_element_type=jnp.float32)
            for chunk in range(chunks):
                at = (part * chunks + chunk) * 32
                kept = jnp.where(member == slot * chunks + chunk, grown, 0.0)
                mix_ref[at : at + seq_rows, :] += kept.astype(jnp.bfloat16)
    for copy in loads[15:]:
        copy.wait()
    for copy in stores:
        copy.wait()


def rows_kernel(
    gathered_ref,
    tokens_ref,
    gain_ref,
    residual_ref,
    input_ref,
    rows_ref,
    sums_v,
    tokens_v,
    wide_v,
):
    seq_rows, width = tokens_ref.shape
    padded = tokens_v.shape[0]
    lanes = width // 128
    core = lax.axis_index("ep") % 2
    slot = lax.axis_index("tp") % 2
    group = gathered_ref.shape[0] // 2
    sent = seq_rows * lanes
    peers = rows_ref.shape[0] // (2 * lanes)
    tokens_v[...] = jnp.zeros(tokens_v.shape, jnp.float32)
    tokens_v[:seq_rows, :] = tokens_ref[...].astype(jnp.float32)
    for place in range(2):
        first = (core if place == 0 else 1 - core) * group
        summed = jnp.sum(gathered_ref[pl.ds(first, group), :sent].astype(jnp.float32), axis=0)
        sums_v[place, :sent] = summed
        sums_v[place, sent:] = jnp.zeros((padded * lanes - sent, 128), jnp.float32)
        total = jnp.concatenate(
            [sums_v[place, pl.ds(lane, padded, stride=lanes), :] for lane in range(lanes)],
            axis=1,
        )
        if place == 0:
            total = tokens_v[...] + total.astype(jnp.bfloat16).astype(jnp.float32)
        names = gathered_ref[first, sent:, :].astype(jnp.float32)
        blank = jnp.zeros((128 - names.shape[0], 128), jnp.float32)
        routes = jnp.concatenate([names, blank], axis=0).T[:padded, :6]
        picks = picked_rows(routes.astype(jnp.int32), core, slot)
        residual = total.astype(jnp.bfloat16)
        inputs = rms_rows(residual.astype(jnp.float32), gain_ref[...]).astype(jnp.bfloat16)
        if place == 0:
            residual_ref[...] = residual[:seq_rows]
            input_ref[...] = inputs[:seq_rows]
        picked = lax.dot_general(
            picks, inputs, (((0,), (0,)), ((), ())), preferred_element_type=jnp.float32
        )
        for lane in range(lanes):
            wide_v[pl.ds(place * lanes + lane, peers, stride=2 * lanes), :] = picked[
                :, lane * 128 : (lane + 1) * 128
            ]
    rows_ref[...] = wide_v[...].astype(jnp.bfloat16)


def unpack_kernel(sent_ref, rows_ref, wide_v):
    lanes = rows_ref.shape[1] // 128
    experts = rows_ref.shape[0]
    wide_v[...] = sent_ref[...].astype(jnp.float32)
    for lane in range(lanes):
        rows_ref[:, lane * 128 : (lane + 1) * 128] = wide_v[
            pl.ds(lane, experts, stride=lanes), :
        ].astype(jnp.bfloat16)


def expert_kernel(rows_ref, own_ref, other_ref, shared_ref, blocks_ref, total_v):
    core = lax.axis_index("ep") % 2
    experts, width = rows_ref.shape
    rows = rows_ref[...]
    acts = []
    for pack_ref in (own_ref, other_ref):
        both = jnp.dot(rows, pack_ref[:width], preferred_element_type=jnp.float32)
        gate, up = both[:, :128], both[:, 128:]
        acts.append((gate / (1.0 + jnp.exp(-gate)) * up).astype(jnp.bfloat16))
    act = jnp.concatenate(acts, axis=1)
    group = blocks_ref.shape[0] // 2
    share = width // group
    peers = experts // 2
    for part in range(group):
        start = width + part * 128
        down = jnp.concatenate([own_ref[start : start + 128], other_ref[start : start + 128]], axis=0)
        total = jnp.dot(act, down, preferred_element_type=jnp.float32)
        for chunk in range(share // 128):
            total_v[chunk] = total[:, chunk * 128 : (chunk + 1) * 128]
        mine, theirs = [
            jnp.concatenate(
                [total_v[chunk, pl.ds(at, peers, stride=2), :] for chunk in range(share // 128)],
                axis=1,
            ).astype(jnp.bfloat16)
            for at in range(2)
        ]
        shared = shared_ref[:, part * share : (part + 1) * share]
        for target in range(2):
            here = core == target
            blocks_ref[target * group + part, :peers, :] = jnp.where(here, mine, theirs)
            blocks_ref[target * group + part, peers:, :] = jnp.where(
                here, shared, jnp.zeros_like(shared)
            )


def share_kernel(parts_ref, rows_ref, shared_ref, wide_v):
    share = parts_ref.shape[2]
    seq_rows = shared_ref.shape[0]
    peers = parts_ref.shape[1] - seq_rows
    group = parts_ref.shape[0] // 2
    chunks = share // 128
    stride = rows_ref.shape[0] // peers
    for source in range(2):
        for slot in range(2):
            total = parts_ref[source * group + slot, :peers, :].astype(jnp.float32)
            total += parts_ref[source * group + slot + 2, :peers, :].astype(jnp.float32)
            for chunk in range(chunks):
                at = (source * 2 + slot) * chunks + chunk
                wide_v[pl.ds(at, peers, stride=stride), :] = total[
                    :, chunk * 128 : (chunk + 1) * 128
                ]
    rows_ref[...] = wide_v[...].astype(jnp.bfloat16)
    shared = jnp.sum(parts_ref[:, peers:, :].astype(jnp.float32), axis=0)
    shared_ref[...] = shared.astype(jnp.bfloat16).astype(jnp.float32)


def final_kernel(rows_ref, mix_ref, residual_ref, shared_ref, out_ref):
    seq_rows, share = out_ref.shape
    chunks = share // 128
    found = jnp.dot(mix_ref[...], rows_ref[...], preferred_element_type=jnp.float32)
    at = pl.multiple_of(lax.axis_index("tp") * share, share)
    base = residual_ref[:, pl.ds(at, share)].astype(jnp.float32) + shared_ref[...]
    for chunk in range(chunks):
        high = found[chunk * 32 : chunk * 32 + seq_rows]
        low = found[(chunks + chunk) * 32 : (chunks + chunk) * 32 + seq_rows]
        total = base[:, chunk * 128 : (chunk + 1) * 128] + (high + low)
        out_ref[:, chunk * 128 : (chunk + 1) * 128] = total.astype(jnp.bfloat16)


def vmem():
    return pl.BlockSpec(memory_space=pltpu.VMEM)


def anywhere():
    return pl.BlockSpec(memory_space=pl.ANY)


def in_vmem(array):
    return pltpu.with_memory_space_constraint(array, pltpu.VMEM)


def per_device(
    tokens,
    delta_state,
    mixer_gain,
    query_weight,
    key_weight,
    value_weight,
    write_weight,
    decay_weight,
    decay_rate,
    decay_bias,
    head_gain,
    out_weight,
    channel_gain,
    routes,
    route_weights,
    expert_gate,
    expert_up,
    expert_down,
    shared_gate,
    shared_up,
    shared_down,
):
    seq_rows, model_width = tokens.shape
    head_dim = delta_state.shape[2]
    tp_count = lax.axis_size("tp")
    ep_count = lax.axis_size("ep")
    share_width = model_width // tp_count
    hidden = expert_gate.shape[2]
    quads = 2 * (share_width // 128)
    lanes = model_width // 128
    sent_rows = seq_rows * lanes + 8
    same_core = [[2 * p + k for p in range(ep_count // 2)] for k in range(2)]
    chips = [
        [(2 * p + k) * tp_count + t for k in range(2) for t in range(tp_count)]
        for p in range(ep_count // 2)
    ]
    f32, bf16 = jnp.float32, jnp.bfloat16
    state = delta_state.reshape(seq_rows, head_dim, head_dim)
    partials, next_state, mix, packed = pl.pallas_call(
        mixer_kernel,
        out_shape=[
            jax.ShapeDtypeStruct((2 * tp_count, sent_rows, 128), bf16),
            jax.ShapeDtypeStruct(state.shape, f32),
            pltpu.VMEM((64 * (share_width // 128), ep_count * quads), bf16),
            pltpu.VMEM((3 * model_width // 2, 2 * hidden), bf16),
        ],
        in_specs=[anywhere()] * 17,
        out_specs=[anywhere()] * 2 + [vmem()] * 2,
        scratch_shapes=[
            pltpu.VMEM((seq_rows, model_width), bf16),
            pltpu.VMEM((1, model_width), f32),
            pltpu.VMEM((1, model_width), bf16),
            pltpu.VMEM((1, model_width), bf16),
            pltpu.VMEM((1, head_dim), f32),
            pltpu.SMEM((1,), f32),
            pltpu.SMEM((1,), f32),
            pltpu.VMEM(routes.T.shape, jnp.int32),
            pltpu.VMEM(routes.T.shape, f32),
            pltpu.VMEM((model_width, head_dim), bf16),
            pltpu.VMEM((model_width, head_dim), bf16),
            pltpu.VMEM((model_width, head_dim), bf16),
            pltpu.VMEM((seq_rows, head_dim, head_dim), f32),
            pltpu.VMEM((seq_rows, head_dim, head_dim), f32),
            pltpu.VMEM((head_dim, model_width), bf16),
            pltpu.VMEM((2 * tp_count, sent_rows, 128), bf16),
            pltpu.VMEM((sent_rows, 128), f32),
            pltpu.VMEM((sent_rows, 128), f32),
            pltpu.VMEM((seq_rows, head_dim), f32),
            pltpu.VMEM((seq_rows, head_dim), f32),
            pltpu.SemaphoreType.DMA((17 + model_width // (2 * hidden),)),
        ],
    )(
        tokens,
        mixer_gain.reshape(1, model_width),
        write_weight.reshape(1, model_width),
        decay_weight.reshape(1, model_width),
        head_gain.reshape(1, head_dim),
        decay_rate,
        decay_bias,
        routes.T,
        route_weights.T,
        query_weight,
        key_weight,
        value_weight,
        state,
        out_weight,
        expert_gate[0],
        expert_up[0],
        expert_down[0],
    )
    gathered = lax.all_to_all(partials, ("ep", "tp"), 0, 0, axis_index_groups=chips, tiled=True)
    other = lax.ppermute(packed, "tp", [(i, i ^ 1) for i in range(tp_count)])
    residual, expert_input, outgoing = pl.pallas_call(
        rows_kernel,
        out_shape=[
            pltpu.VMEM((seq_rows, model_width), bf16),
            pltpu.VMEM((seq_rows, model_width), bf16),
            pltpu.VMEM((ep_count * lanes, 128), bf16),
        ],
        in_specs=[vmem()] * 3,
        out_specs=[vmem()] * 3,
        scratch_shapes=[
            pltpu.VMEM((2, 32 * lanes, 128), f32),
            pltpu.VMEM((32, model_width), f32),
            pltpu.VMEM((ep_count * lanes, 128), f32),
        ],
    )(
        in_vmem(gathered),
        in_vmem(tokens),
        in_vmem(channel_gain.reshape(1, model_width)),
    )
    shared_act = (
        jax.nn.silu(jnp.dot(expert_input, shared_gate, preferred_element_type=f32))
        * jnp.dot(expert_input, shared_up, preferred_element_type=f32)
    ).astype(bf16)
    shared_partial = jnp.dot(shared_act, shared_down, preferred_element_type=f32).astype(bf16)
    outgoing, shared_partial = lax.optimization_barrier((outgoing, shared_partial))
    received = lax.all_to_all(
        outgoing.reshape(ep_count // 2, 2 * lanes, 128),
        "ep",
        0,
        0,
        axis_index_groups=same_core,
        tiled=True,
    )
    rows = pl.pallas_call(
        unpack_kernel,
        out_shape=pltpu.VMEM((ep_count, model_width), bf16),
        in_specs=[vmem()],
        out_specs=vmem(),
        scratch_shapes=[pltpu.VMEM((ep_count * lanes, 128), f32)],
    )(in_vmem(received.reshape(ep_count * lanes, 128)))
    blocks = pl.pallas_call(
        expert_kernel,
        out_shape=pltpu.VMEM((2 * tp_count, ep_count // 2 + seq_rows, share_width), bf16),
        in_specs=[vmem()] * 4,
        out_specs=vmem(),
        scratch_shapes=[
            pltpu.VMEM((share_width // 128, ep_count, 128), f32),
        ],
    )(
        in_vmem(rows),
        in_vmem(packed),
        in_vmem(other),
        in_vmem(shared_partial),
    )
    parts = lax.all_to_all(
        blocks, ("ep", "tp"), 0, 0, axis_index_groups=chips, tiled=True
    )
    expert_share, shared_out = pl.pallas_call(
        share_kernel,
        out_shape=[
            pltpu.VMEM((ep_count * quads, 128), bf16),
            pltpu.VMEM((seq_rows, share_width), f32),
        ],
        in_specs=[vmem()],
        out_specs=[vmem()] * 2,
        scratch_shapes=[pltpu.VMEM((ep_count * quads, 128), f32)],
    )(in_vmem(parts))
    returned = lax.all_to_all(
        expert_share.reshape(ep_count // 2, 2 * quads, 128),
        "ep",
        0,
        0,
        axis_index_groups=same_core,
        tiled=True,
    )
    layer_out = pl.pallas_call(
        final_kernel,
        out_shape=jax.ShapeDtypeStruct((seq_rows, share_width), bf16),
        in_specs=[vmem()] * 4,
        out_specs=vmem(),
    )(
        in_vmem(returned.reshape(ep_count * quads, 128)),
        in_vmem(mix),
        in_vmem(residual),
        in_vmem(shared_out),
    )
    return (layer_out, next_state.reshape(delta_state.shape))


def solution(mesh):
    return jax.shard_map(
        per_device,
        mesh=mesh,
        in_specs=(
            P("ep", None),
            P("ep", "tp", None, None),
            P(),
            P(None, "tp"),
            P(None, "tp"),
            P(None, "tp"),
            P(None, "tp"),
            P(None, "tp"),
            P("tp"),
            P("tp"),
            P(),
            P("tp", None),
            P(),
            P("ep", None),
            P("ep", None),
            P("ep", None, "tp"),
            P("ep", None, "tp"),
            P("ep", "tp", None),
            P(None, "tp"),
            P(None, "tp"),
            P("tp", None),
        ),
        out_specs=(P("ep", "tp"), P("ep", "tp", None, None)),
        check_vma=False,
    )
```

```python
import jax
import jax.numpy as jnp
from jax import lax
from jax.experimental import pallas as pl
from jax.experimental.pallas import tpu as pltpu
from jax.sharding import PartitionSpec as P

EPS = 1e-06
ROUTED_SCALE = 2.5


def rms_rows(values, gain_vec):
    mean_square = jnp.mean(values * values, axis=-1, keepdims=True)
    return values * lax.rsqrt(mean_square + EPS) * gain_vec


def unit_rows(raw):
    vals = raw.astype(jnp.bfloat16).astype(jnp.float32)
    return vals * lax.rsqrt(jnp.sum(vals * vals, axis=-1, keepdims=True) + EPS)


def columns_of(rows):
    pad = jnp.zeros((128 - rows.shape[0], rows.shape[1]), rows.dtype)
    return jnp.concatenate([rows, pad], axis=0).T


def earlier_rows(named):
    seq_rows = named.shape[0]
    row_a = lax.broadcasted_iota(jnp.int32, (seq_rows, seq_rows), 0)
    row_b = lax.broadcasted_iota(jnp.int32, (seq_rows, seq_rows), 1)
    below = jnp.where(row_b < row_a, 1.0, 0.0)
    return jnp.dot(below, named, preferred_element_type=jnp.float32).astype(jnp.int32)


def picked_rows(routes, core, slot):
    seq_rows, top_k = routes.shape
    experts = 2 * lax.broadcasted_iota(jnp.int32, (seq_rows, 64), 1) + core
    named = jnp.zeros((seq_rows, 64), jnp.float32)
    for route in range(top_k):
        named = named + jnp.where(experts == routes[:, route : route + 1], 1.0, 0.0)
    return jnp.where(earlier_rows(named) == slot, named, 0.0).astype(jnp.bfloat16)


def mixer_kernel(
    tokens_hbm,
    gain_hbm,
    write_hbm,
    decay_hbm,
    head_gain_hbm,
    rate_hbm,
    bias_hbm,
    routes_hbm,
    weights_hbm,
    query_hbm,
    key_hbm,
    value_hbm,
    state_hbm,
    out_weight_hbm,
    gate_hbm,
    up_hbm,
    down_hbm,
    partial_hbm,
    key_unit_ref,
    update_ref,
    keep_ref,
    packed_ref,
    tokens_v,
    gain_v,
    write_v,
    decay_v,
    head_gain_v,
    rate_v,
    bias_v,
    routes_v,
    weights_v,
    query_v,
    key_v,
    value_v,
    state_v,
    out_weight_v,
    partial_v,
    plain_v,
    mixed_v,
    found_k,
    found_q,
    sems,
):
    seq_rows = tokens_hbm.shape[0]
    core = lax.axis_index("ep") % 2
    tp_index = lax.axis_index("tp")
    width, hidden = gate_hbm.shape
    half = seq_rows // 2
    wide_block = 2 * hidden
    pairs = [
        (tokens_hbm, tokens_v),
        (gain_hbm, gain_v),
        (write_hbm, write_v),
        (decay_hbm, decay_v),
        (rate_hbm, rate_v),
        (bias_hbm, bias_v),
        (routes_hbm, routes_v),
        (weights_hbm, weights_v),
        (query_hbm, query_v),
        (key_hbm, key_v),
        (value_hbm, value_v),
        (state_hbm.at[pl.ds(0, half)], state_v.at[pl.ds(0, half)]),
        (
            state_hbm.at[pl.ds(half, seq_rows - half)],
            state_v.at[pl.ds(half, seq_rows - half)],
        ),
        (head_gain_hbm, head_gain_v),
        (out_weight_hbm, out_weight_v),
        (gate_hbm, packed_ref.at[pl.ds(0, width), pl.ds(0, hidden)]),
        (up_hbm, packed_ref.at[pl.ds(0, width), pl.ds(hidden, hidden)]),
    ] + [
        (
            down_hbm.at[:, pl.ds(j * wide_block, wide_block)],
            packed_ref.at[pl.ds(width + j * hidden, hidden)],
        )
        for j in range(width // wide_block)
    ]
    loads = [pltpu.make_async_copy(src, dst, sems.at[i]) for i, (src, dst) in enumerate(pairs)]
    for copy in loads:
        copy.start()
    for copy in loads[:8]:
        copy.wait()
    normed = rms_rows(tokens_v[...].astype(jnp.float32), gain_v[...]).astype(jnp.bfloat16)
    wide = normed.astype(jnp.float32)
    write_logit = jnp.sum(wide * write_v[...].astype(jnp.float32), axis=-1, keepdims=True)
    decay_logit = jnp.sum(wide * decay_v[...].astype(jnp.float32), axis=-1, keepdims=True)
    write_rate = 1.0 / (1.0 + jnp.exp(-write_logit))
    biased = decay_logit + bias_v[0]
    softplus = jnp.maximum(biased, 0.0) + jnp.log1p(jnp.exp(-jnp.abs(biased)))
    keep = jnp.exp(-rate_v[0] * softplus)
    loads[8].wait()
    query_raw = jnp.dot(normed, query_v[...], preferred_element_type=jnp.float32)
    loads[9].wait()
    key_raw = jnp.dot(normed, key_v[...], preferred_element_type=jnp.float32)
    loads[10].wait()
    value_raw = jnp.dot(normed, value_v[...], preferred_element_type=jnp.float32)
    query_unit = unit_rows(query_raw) * query_raw.shape[1] ** (-0.5)
    key_unit = unit_rows(key_raw)
    value_vec = value_raw.astype(jnp.bfloat16).astype(jnp.float32)
    key_cols = columns_of(key_unit)
    query_cols = columns_of(query_unit)
    for row in range(seq_rows):
        if row == 0:
            loads[11].wait()
        if row == half:
            loads[12].wait()
        state = state_v[row]
        found_k[row : row + 1, :] = jnp.sum(
            state * key_cols[:, row : row + 1], axis=0, keepdims=True
        )
        found_q[row : row + 1, :] = jnp.sum(
            state * query_cols[:, row : row + 1], axis=0, keepdims=True
        )
    loads[13].wait()
    correction = value_vec - keep * found_k[...]
    overlap = jnp.sum(key_unit * query_unit, axis=-1, keepdims=True)
    update = write_rate * correction
    readout = keep * found_q[...] + overlap * update
    head_out = rms_rows(readout, head_gain_v[...]).astype(jnp.bfloat16)
    loads[14].wait()
    partial = jnp.dot(head_out, out_weight_v[...], preferred_element_type=jnp.float32)
    partial = partial.astype(jnp.bfloat16).astype(jnp.float32)
    mixed = partial + jnp.where(tp_index == 0, tokens_v[...].astype(jnp.float32), 0.0)
    lanes = width // 128
    top_k = routes_hbm.shape[0]
    for lane in range(lanes):
        part = slice(lane * 128, (lane + 1) * 128)
        plain_v[pl.ds(lane, seq_rows, stride=lanes), :] = partial[:, part]
        mixed_v[pl.ds(lane, seq_rows, stride=lanes), :] = mixed[:, part]
    plain_v[seq_rows * lanes :, :] = jnp.zeros((8, 128), jnp.float32)
    mixed_v[seq_rows * lanes :, :] = jnp.zeros((8, 128), jnp.float32)
    names = slice(seq_rows * lanes, seq_rows * lanes + top_k)
    plain_v[names, :seq_rows] = routes_v[...].astype(jnp.float32)
    mixed_v[names, :seq_rows] = routes_v[...].astype(jnp.float32)
    plain = plain_v[...].astype(jnp.bfloat16)
    mixed = mixed_v[...].astype(jnp.bfloat16)
    group = partial_v.shape[0] // 2
    for copy_number in range(partial_v.shape[0]):
        partial_v[copy_number] = jnp.where(core == copy_number // group, plain, mixed)
    store = pltpu.make_async_copy(partial_v, partial_hbm, sems.at[0])
    store.start()
    key_unit_ref[...] = key_unit
    update_ref[...] = update
    keep_ref[...] = jnp.broadcast_to(keep, keep_ref.shape)
    for copy in loads[15:]:
        copy.wait()
    store.wait()


def state_kernel(
    routes_ref,
    weights_ref,
    key_unit_ref,
    update_ref,
    keep_ref,
    state_hbm,
    next_hbm,
    mix_ref,
    state_v,
    next_v,
    sems,
):
    seq_rows = key_unit_ref.shape[0]
    half = seq_rows // 2
    spans = [(0, half), (half, seq_rows - half)]
    loads = [
        pltpu.make_async_copy(
            state_hbm.at[pl.ds(at, size)], state_v.at[pl.ds(at, size)], sems.at[i]
        )
        for i, (at, size) in enumerate(spans)
    ]
    stores = [
        pltpu.make_async_copy(
            next_v.at[pl.ds(at, size)], next_hbm.at[pl.ds(at, size)], sems.at[2 + i]
        )
        for i, (at, size) in enumerate(spans)
    ]
    for copy in loads:
        copy.start()
    routes = columns_of(routes_ref[...].astype(jnp.float32))[:seq_rows].astype(jnp.int32)
    weights = columns_of(weights_ref[...])[:seq_rows]
    scale = weights / jnp.sum(weights, axis=1, keepdims=True) * ROUTED_SCALE
    expert_iota = lax.broadcasted_iota(jnp.int32, (seq_rows, 128), 1)
    named = jnp.zeros((seq_rows, 128), jnp.float32)
    mix = jnp.zeros((seq_rows, 128), jnp.float32)
    for route in range(routes_ref.shape[0]):
        hit = expert_iota == routes[:, route : route + 1]
        named = named + jnp.where(hit, 1.0, 0.0)
        mix = mix + jnp.where(hit, scale[:, route : route + 1], 0.0)
    chosen = earlier_rows(named)
    slots, experts = 2, 128
    chunks = mix_ref.shape[0] // 64
    spread = slots * chunks * experts
    lane = lax.broadcasted_iota(jnp.int32, (experts, spread), 1)
    place = lax.broadcasted_iota(jnp.int32, (experts, spread), 0)
    expand = jnp.where(lane // (slots * chunks) == place, 1.0, 0.0).astype(jnp.bfloat16)
    member = lax.broadcasted_iota(jnp.int32, (seq_rows, spread), 1) % (slots * chunks)
    mix_ref[...] = jnp.zeros(mix_ref.shape, mix_ref.dtype)
    for slot in range(slots):
        full = jnp.where(chosen == slot, mix, 0.0)
        high = full.astype(jnp.bfloat16)
        low = (full - high.astype(jnp.float32)).astype(jnp.bfloat16)
        for part, term in enumerate((high, low)):
            grown = jnp.dot(term, expand, preferred_element_type=jnp.float32)
            for chunk in range(chunks):
                at = (part * chunks + chunk) * 32
                kept = jnp.where(member == slot * chunks + chunk, grown, 0.0)
                mix_ref[at : at + seq_rows, :] += kept.astype(jnp.bfloat16)
    key_cols = columns_of(key_unit_ref[...])
    for part, (at, size) in enumerate(spans):
        loads[part].wait()
        for row in range(at, at + size):
            next_v[row] = (
                keep_ref[row : row + 1, :] * state_v[row]
                + key_cols[:, row : row + 1] * update_ref[row : row + 1, :]
            )
        stores[part].start()
    for copy in stores:
        copy.wait()


def rows_kernel(
    gathered_ref,
    tokens_ref,
    gain_ref,
    residual_ref,
    input_ref,
    rows_ref,
    sums_v,
    tokens_v,
    wide_v,
):
    seq_rows, width = tokens_ref.shape
    padded = tokens_v.shape[0]
    lanes = width // 128
    core = lax.axis_index("ep") % 2
    slot = lax.axis_index("tp") % 2
    group = gathered_ref.shape[0] // 2
    sent = seq_rows * lanes
    peers = rows_ref.shape[0] // (2 * lanes)
    tokens_v[...] = jnp.zeros(tokens_v.shape, jnp.float32)
    tokens_v[:seq_rows, :] = tokens_ref[...].astype(jnp.float32)
    for place in range(2):
        first = (core if place == 0 else 1 - core) * group
        summed = jnp.sum(gathered_ref[pl.ds(first, group), :sent].astype(jnp.float32), axis=0)
        sums_v[place, :sent] = summed
        sums_v[place, sent:] = jnp.zeros((padded * lanes - sent, 128), jnp.float32)
        total = jnp.concatenate(
            [sums_v[place, pl.ds(lane, padded, stride=lanes), :] for lane in range(lanes)],
            axis=1,
        )
        if place == 0:
            total = tokens_v[...] + total.astype(jnp.bfloat16).astype(jnp.float32)
        names = gathered_ref[first, sent:, :].astype(jnp.float32)
        blank = jnp.zeros((128 - names.shape[0], 128), jnp.float32)
        routes = jnp.concatenate([names, blank], axis=0).T[:padded, :6]
        picks = picked_rows(routes.astype(jnp.int32), core, slot)
        residual = total.astype(jnp.bfloat16)
        inputs = rms_rows(residual.astype(jnp.float32), gain_ref[...]).astype(jnp.bfloat16)
        if place == 0:
            residual_ref[...] = residual[:seq_rows]
            input_ref[...] = inputs[:seq_rows]
        picked = lax.dot_general(
            picks, inputs, (((0,), (0,)), ((), ())), preferred_element_type=jnp.float32
        )
        for lane in range(lanes):
            wide_v[pl.ds(place * lanes + lane, peers, stride=2 * lanes), :] = picked[
                :, lane * 128 : (lane + 1) * 128
            ]
    rows_ref[...] = wide_v[...].astype(jnp.bfloat16)


def unpack_kernel(sent_ref, rows_ref, wide_v):
    lanes = rows_ref.shape[1] // 128
    experts = rows_ref.shape[0]
    wide_v[...] = sent_ref[...].astype(jnp.float32)
    for lane in range(lanes):
        rows_ref[:, lane * 128 : (lane + 1) * 128] = wide_v[
            pl.ds(lane, experts, stride=lanes), :
        ].astype(jnp.bfloat16)


def expert_kernel(rows_ref, own_ref, other_ref, shared_ref, blocks_ref, total_v):
    core = lax.axis_index("ep") % 2
    experts, width = rows_ref.shape
    rows = rows_ref[...]
    acts = []
    for pack_ref in (own_ref, other_ref):
        both = jnp.dot(rows, pack_ref[:width], preferred_element_type=jnp.float32)
        gate, up = both[:, :128], both[:, 128:]
        acts.append((gate / (1.0 + jnp.exp(-gate)) * up).astype(jnp.bfloat16))
    act = jnp.concatenate(acts, axis=1)
    group = blocks_ref.shape[0] // 2
    share = width // group
    peers = experts // 2
    for part in range(group):
        start = width + part * 128
        down = jnp.concatenate([own_ref[start : start + 128], other_ref[start : start + 128]], axis=0)
        total = jnp.dot(act, down, preferred_element_type=jnp.float32)
        for chunk in range(share // 128):
            total_v[chunk] = total[:, chunk * 128 : (chunk + 1) * 128]
        mine, theirs = [
            jnp.concatenate(
                [total_v[chunk, pl.ds(at, peers, stride=2), :] for chunk in range(share // 128)],
                axis=1,
            ).astype(jnp.bfloat16)
            for at in range(2)
        ]
        shared = shared_ref[:, part * share : (part + 1) * share]
        for target in range(2):
            here = core == target
            blocks_ref[target * group + part, :peers, :] = jnp.where(here, mine, theirs)
            blocks_ref[target * group + part, peers:, :] = jnp.where(
                here, shared, jnp.zeros_like(shared)
            )


def share_kernel(parts_ref, rows_ref, shared_ref, wide_v):
    share = parts_ref.shape[2]
    seq_rows = shared_ref.shape[0]
    peers = parts_ref.shape[1] - seq_rows
    group = parts_ref.shape[0] // 2
    chunks = share // 128
    stride = rows_ref.shape[0] // peers
    for source in range(2):
        for slot in range(2):
            total = parts_ref[source * group + slot, :peers, :].astype(jnp.float32)
            total += parts_ref[source * group + slot + 2, :peers, :].astype(jnp.float32)
            for chunk in range(chunks):
                at = (source * 2 + slot) * chunks + chunk
                wide_v[pl.ds(at, peers, stride=stride), :] = total[
                    :, chunk * 128 : (chunk + 1) * 128
                ]
    rows_ref[...] = wide_v[...].astype(jnp.bfloat16)
    shared = jnp.sum(parts_ref[:, peers:, :].astype(jnp.float32), axis=0)
    shared_ref[...] = shared.astype(jnp.bfloat16).astype(jnp.float32)


def final_kernel(rows_ref, mix_ref, residual_ref, shared_ref, out_ref):
    seq_rows, share = out_ref.shape
    chunks = share // 128
    found = jnp.dot(mix_ref[...], rows_ref[...], preferred_element_type=jnp.float32)
    at = pl.multiple_of(lax.axis_index("tp") * share, share)
    base = residual_ref[:, pl.ds(at, share)].astype(jnp.float32) + shared_ref[...]
    for chunk in range(chunks):
        high = found[chunk * 32 : chunk * 32 + seq_rows]
        low = found[(chunks + chunk) * 32 : (chunks + chunk) * 32 + seq_rows]
        total = base[:, chunk * 128 : (chunk + 1) * 128] + (high + low)
        out_ref[:, chunk * 128 : (chunk + 1) * 128] = total.astype(jnp.bfloat16)


def vmem():
    return pl.BlockSpec(memory_space=pltpu.VMEM)


def anywhere():
    return pl.BlockSpec(memory_space=pl.ANY)


def in_vmem(array):
    return pltpu.with_memory_space_constraint(array, pltpu.VMEM)


def per_device(
    tokens,
    delta_state,
    mixer_gain,
    query_weight,
    key_weight,
    value_weight,
    write_weight,
    decay_weight,
    decay_rate,
    decay_bias,
    head_gain,
    out_weight,
    channel_gain,
    routes,
    route_weights,
    expert_gate,
    expert_up,
    expert_down,
    shared_gate,
    shared_up,
    shared_down,
):
    seq_rows, model_width = tokens.shape
    head_dim = delta_state.shape[2]
    tp_count = lax.axis_size("tp")
    ep_count = lax.axis_size("ep")
    share_width = model_width // tp_count
    hidden = expert_gate.shape[2]
    quads = 2 * (share_width // 128)
    lanes = model_width // 128
    sent_rows = seq_rows * lanes + 8
    same_core = [[2 * p + k for p in range(ep_count // 2)] for k in range(2)]
    chips = [
        [(2 * p + k) * tp_count + t for k in range(2) for t in range(tp_count)]
        for p in range(ep_count // 2)
    ]
    f32, bf16 = jnp.float32, jnp.bfloat16
    state = delta_state.reshape(seq_rows, head_dim, head_dim)
    small = pltpu.VMEM((seq_rows, head_dim), f32)
    partials, key_unit, update, keep, packed = pl.pallas_call(
        mixer_kernel,
        out_shape=[
            jax.ShapeDtypeStruct((2 * tp_count, sent_rows, 128), bf16),
            small,
            small,
            small,
            pltpu.VMEM((3 * model_width // 2, 2 * hidden), bf16),
        ],
        in_specs=[anywhere()] * 17,
        out_specs=[anywhere()] + [vmem()] * 4,
        scratch_shapes=[
            pltpu.VMEM((seq_rows, model_width), bf16),
            pltpu.VMEM((1, model_width), f32),
            pltpu.VMEM((1, model_width), bf16),
            pltpu.VMEM((1, model_width), bf16),
            pltpu.VMEM((1, head_dim), f32),
            pltpu.SMEM((1,), f32),
            pltpu.SMEM((1,), f32),
            pltpu.VMEM(routes.T.shape, jnp.int32),
            pltpu.VMEM(routes.T.shape, f32),
            pltpu.VMEM((model_width, head_dim), bf16),
            pltpu.VMEM((model_width, head_dim), bf16),
            pltpu.VMEM((model_width, head_dim), bf16),
            pltpu.VMEM((seq_rows, head_dim, head_dim), f32),
            pltpu.VMEM((head_dim, model_width), bf16),
            pltpu.VMEM((2 * tp_count, sent_rows, 128), bf16),
            pltpu.VMEM((sent_rows, 128), f32),
            pltpu.VMEM((sent_rows, 128), f32),
            pltpu.VMEM((seq_rows, head_dim), f32),
            pltpu.VMEM((seq_rows, head_dim), f32),
            pltpu.SemaphoreType.DMA((17 + model_width // (2 * hidden),)),
        ],
    )(
        tokens,
        mixer_gain.reshape(1, model_width),
        write_weight.reshape(1, model_width),
        decay_weight.reshape(1, model_width),
        head_gain.reshape(1, head_dim),
        decay_rate,
        decay_bias,
        routes.T,
        route_weights.T,
        query_weight,
        key_weight,
        value_weight,
        state,
        out_weight,
        expert_gate[0],
        expert_up[0],
        expert_down[0],
    )
    gathered = lax.all_to_all(
        partials, ("ep", "tp"), 0, 0, axis_index_groups=chips, tiled=True
    )
    next_state, mix = pl.pallas_call(
        state_kernel,
        out_shape=[
            jax.ShapeDtypeStruct(state.shape, f32),
            pltpu.VMEM((64 * (share_width // 128), ep_count * quads), bf16),
        ],
        in_specs=[vmem()] * 5 + [anywhere()],
        out_specs=[anywhere(), vmem()],
        scratch_shapes=[
            pltpu.VMEM(state.shape, f32),
            pltpu.VMEM(state.shape, f32),
            pltpu.SemaphoreType.DMA((4,)),
        ],
    )(
        in_vmem(routes.T),
        in_vmem(route_weights.T),
        in_vmem(key_unit),
        in_vmem(update),
        in_vmem(keep),
        state,
    )
    other = lax.ppermute(packed, "tp", [(i, i ^ 1) for i in range(tp_count)])
    residual, expert_input, outgoing = pl.pallas_call(
        rows_kernel,
        out_shape=[
            pltpu.VMEM((seq_rows, model_width), bf16),
            pltpu.VMEM((seq_rows, model_width), bf16),
            pltpu.VMEM((ep_count * lanes, 128), bf16),
        ],
        in_specs=[vmem()] * 3,
        out_specs=[vmem()] * 3,
        scratch_shapes=[
            pltpu.VMEM((2, 32 * lanes, 128), f32),
            pltpu.VMEM((32, model_width), f32),
            pltpu.VMEM((ep_count * lanes, 128), f32),
        ],
    )(in_vmem(gathered), in_vmem(tokens), in_vmem(channel_gain.reshape(1, model_width)))
    shared_act = (
        jax.nn.silu(jnp.dot(expert_input, shared_gate, preferred_element_type=f32))
        * jnp.dot(expert_input, shared_up, preferred_element_type=f32)
    ).astype(bf16)
    shared_partial = jnp.dot(shared_act, shared_down, preferred_element_type=f32).astype(bf16)
    outgoing, shared_partial = lax.optimization_barrier((outgoing, shared_partial))
    received = lax.all_to_all(
        outgoing.reshape(ep_count // 2, 2 * lanes, 128),
        "ep",
        0,
        0,
        axis_index_groups=same_core,
        tiled=True,
    )
    rows = pl.pallas_call(
        unpack_kernel,
        out_shape=pltpu.VMEM((ep_count, model_width), bf16),
        in_specs=[vmem()],
        out_specs=vmem(),
        scratch_shapes=[pltpu.VMEM((ep_count * lanes, 128), f32)],
    )(in_vmem(received.reshape(ep_count * lanes, 128)))
    blocks = pl.pallas_call(
        expert_kernel,
        out_shape=pltpu.VMEM((2 * tp_count, ep_count // 2 + seq_rows, share_width), bf16),
        in_specs=[vmem()] * 4,
        out_specs=vmem(),
        scratch_shapes=[
            pltpu.VMEM((share_width // 128, ep_count, 128), f32),
        ],
    )(
        in_vmem(rows),
        in_vmem(packed),
        in_vmem(other),
        in_vmem(shared_partial),
    )
    parts = lax.all_to_all(
        blocks, ("ep", "tp"), 0, 0, axis_index_groups=chips, tiled=True
    )
    expert_share, shared_out = pl.pallas_call(
        share_kernel,
        out_shape=[
            pltpu.VMEM((ep_count * quads, 128), bf16),
            pltpu.VMEM((seq_rows, share_width), f32),
        ],
        in_specs=[vmem()],
        out_specs=[vmem()] * 2,
        scratch_shapes=[pltpu.VMEM((ep_count * quads, 128), f32)],
    )(in_vmem(parts))
    returned = lax.all_to_all(
        expert_share.reshape(ep_count // 2, 2 * quads, 128),
        "ep",
        0,
        0,
        axis_index_groups=same_core,
        tiled=True,
    )
    layer_out = pl.pallas_call(
        final_kernel,
        out_shape=jax.ShapeDtypeStruct((seq_rows, share_width), bf16),
        in_specs=[vmem()] * 4,
        out_specs=vmem(),
    )(
        in_vmem(returned.reshape(ep_count * quads, 128)),
        in_vmem(mix),
        in_vmem(residual),
        in_vmem(shared_out),
    )
    return (layer_out, next_state.reshape(delta_state.shape))


def solution(mesh):
    return jax.shard_map(
        per_device,
        mesh=mesh,
        in_specs=(
            P("ep", None),
            P("ep", "tp", None, None),
            P(),
            P(None, "tp"),
            P(None, "tp"),
            P(None, "tp"),
            P(None, "tp"),
            P(None, "tp"),
            P("tp"),
            P("tp"),
            P(),
            P("tp", None),
            P(),
            P("ep", None),
            P("ep", None),
            P("ep", None, "tp"),
            P("ep", None, "tp"),
            P("ep", "tp", None),
            P(None, "tp"),
            P(None, "tp"),
            P("tp", None),
        ),
        out_specs=(P("ep", "tp"), P("ep", "tp", None, None)),
        check_vma=False,
    )
```

```python
import jax
import jax.numpy as jnp
from jax import lax
from jax.experimental import pallas as pl
from jax.experimental.pallas import tpu as pltpu
from jax.sharding import PartitionSpec as P

EPS = 1e-06
ROUTED_SCALE = 2.5


def rms_rows(values, gain_vec):
    mean_square = jnp.mean(values * values, axis=-1, keepdims=True)
    return values * lax.rsqrt(mean_square + EPS) * gain_vec


def unit_rows(raw):
    vals = raw.astype(jnp.bfloat16).astype(jnp.float32)
    return vals * lax.rsqrt(jnp.sum(vals * vals, axis=-1, keepdims=True) + EPS)


def columns_of(rows):
    pad = jnp.zeros((128 - rows.shape[0], rows.shape[1]), rows.dtype)
    return jnp.concatenate([rows, pad], axis=0).T


def earlier_rows(named):
    seq_rows = named.shape[0]
    row_a = lax.broadcasted_iota(jnp.int32, (seq_rows, seq_rows), 0)
    row_b = lax.broadcasted_iota(jnp.int32, (seq_rows, seq_rows), 1)
    below = jnp.where(row_b < row_a, 1.0, 0.0)
    return jnp.dot(below, named, preferred_element_type=jnp.float32).astype(jnp.int32)


def picked_rows(routes, core, slot):
    seq_rows, top_k = routes.shape
    experts = 2 * lax.broadcasted_iota(jnp.int32, (seq_rows, 64), 1) + core
    named = jnp.zeros((seq_rows, 64), jnp.float32)
    for route in range(top_k):
        named = named + jnp.where(experts == routes[:, route : route + 1], 1.0, 0.0)
    return jnp.where(earlier_rows(named) == slot, named, 0.0).astype(jnp.bfloat16)


def mixer_kernel(
    tokens_hbm,
    gain_hbm,
    write_hbm,
    decay_hbm,
    head_gain_hbm,
    rate_hbm,
    bias_hbm,
    routes_hbm,
    weights_hbm,
    query_hbm,
    key_hbm,
    value_hbm,
    state_hbm,
    out_weight_hbm,
    gate_hbm,
    up_hbm,
    down_hbm,
    partial_hbm,
    key_unit_ref,
    update_ref,
    keep_ref,
    packed_ref,
    tokens_v,
    gain_v,
    write_v,
    decay_v,
    head_gain_v,
    rate_v,
    bias_v,
    routes_v,
    weights_v,
    query_v,
    key_v,
    value_v,
    state_v,
    out_weight_v,
    partial_v,
    plain_v,
    mixed_v,
    found_k,
    found_q,
    sems,
):
    seq_rows = tokens_hbm.shape[0]
    core = lax.axis_index("ep") % 2
    tp_index = lax.axis_index("tp")
    width, hidden = gate_hbm.shape
    half = seq_rows // 2
    wide_block = 2 * hidden
    pairs = [
        (tokens_hbm, tokens_v),
        (gain_hbm, gain_v),
        (write_hbm, write_v),
        (decay_hbm, decay_v),
        (rate_hbm, rate_v),
        (bias_hbm, bias_v),
        (routes_hbm, routes_v),
        (weights_hbm, weights_v),
        (query_hbm, query_v),
        (key_hbm, key_v),
        (value_hbm, value_v),
        (state_hbm.at[pl.ds(0, half)], state_v.at[pl.ds(0, half)]),
        (
            state_hbm.at[pl.ds(half, seq_rows - half)],
            state_v.at[pl.ds(half, seq_rows - half)],
        ),
        (head_gain_hbm, head_gain_v),
        (out_weight_hbm, out_weight_v),
        (gate_hbm, packed_ref.at[pl.ds(0, width), pl.ds(0, hidden)]),
        (up_hbm, packed_ref.at[pl.ds(0, width), pl.ds(hidden, hidden)]),
    ] + [
        (
            down_hbm.at[:, pl.ds(j * wide_block, wide_block)],
            packed_ref.at[pl.ds(width + j * hidden, hidden)],
        )
        for j in range(width // wide_block)
    ]
    loads = [pltpu.make_async_copy(src, dst, sems.at[i]) for i, (src, dst) in enumerate(pairs)]
    for copy in loads:
        copy.start()
    for copy in loads[:8]:
        copy.wait()
    normed = rms_rows(tokens_v[...].astype(jnp.float32), gain_v[...]).astype(jnp.bfloat16)
    wide = normed.astype(jnp.float32)
    write_logit = jnp.sum(wide * write_v[...].astype(jnp.float32), axis=-1, keepdims=True)
    decay_logit = jnp.sum(wide * decay_v[...].astype(jnp.float32), axis=-1, keepdims=True)
    write_rate = 1.0 / (1.0 + jnp.exp(-write_logit))
    biased = decay_logit + bias_v[0]
    softplus = jnp.maximum(biased, 0.0) + jnp.log1p(jnp.exp(-jnp.abs(biased)))
    keep = jnp.exp(-rate_v[0] * softplus)
    loads[8].wait()
    query_raw = jnp.dot(normed, query_v[...], preferred_element_type=jnp.float32)
    loads[9].wait()
    key_raw = jnp.dot(normed, key_v[...], preferred_element_type=jnp.float32)
    loads[10].wait()
    value_raw = jnp.dot(normed, value_v[...], preferred_element_type=jnp.float32)
    query_unit = unit_rows(query_raw) * query_raw.shape[1] ** (-0.5)
    key_unit = unit_rows(key_raw)
    value_vec = value_raw.astype(jnp.bfloat16).astype(jnp.float32)
    key_cols = columns_of(key_unit)
    query_cols = columns_of(query_unit)
    for row in range(seq_rows):
        if row == 0:
            loads[11].wait()
        if row == half:
            loads[12].wait()
        state = state_v[row]
        found_k[row : row + 1, :] = jnp.sum(
            state * key_cols[:, row : row + 1], axis=0, keepdims=True
        )
        found_q[row : row + 1, :] = jnp.sum(
            state * query_cols[:, row : row + 1], axis=0, keepdims=True
        )
    loads[13].wait()
    correction = value_vec - keep * found_k[...]
    overlap = jnp.sum(key_unit * query_unit, axis=-1, keepdims=True)
    update = write_rate * correction
    readout = keep * found_q[...] + overlap * update
    head_out = rms_rows(readout, head_gain_v[...]).astype(jnp.bfloat16)
    loads[14].wait()
    partial = jnp.dot(head_out, out_weight_v[...], preferred_element_type=jnp.float32)
    partial = partial.astype(jnp.bfloat16).astype(jnp.float32)
    mixed = partial + jnp.where(tp_index == 0, tokens_v[...].astype(jnp.float32), 0.0)
    lanes = width // 128
    top_k = routes_hbm.shape[0]
    for lane in range(lanes):
        part = slice(lane * 128, (lane + 1) * 128)
        plain_v[pl.ds(lane, seq_rows, stride=lanes), :] = partial[:, part]
        mixed_v[pl.ds(lane, seq_rows, stride=lanes), :] = mixed[:, part]
    plain_v[seq_rows * lanes :, :] = jnp.zeros((8, 128), jnp.float32)
    mixed_v[seq_rows * lanes :, :] = jnp.zeros((8, 128), jnp.float32)
    names = slice(seq_rows * lanes, seq_rows * lanes + top_k)
    plain_v[names, :seq_rows] = routes_v[...].astype(jnp.float32)
    mixed_v[names, :seq_rows] = routes_v[...].astype(jnp.float32)
    plain = plain_v[...].astype(jnp.bfloat16)
    mixed = mixed_v[...].astype(jnp.bfloat16)
    group = partial_v.shape[0] // 2
    for copy_number in range(partial_v.shape[0]):
        partial_v[copy_number] = jnp.where(core == copy_number // group, plain, mixed)
    store = pltpu.make_async_copy(partial_v, partial_hbm, sems.at[0])
    store.start()
    key_unit_ref[...] = key_unit
    update_ref[...] = update
    keep_ref[...] = jnp.broadcast_to(keep, keep_ref.shape)
    for copy in loads[15:]:
        copy.wait()
    store.wait()


def state_kernel(
    routes_ref,
    weights_ref,
    key_unit_ref,
    update_ref,
    keep_ref,
    state_hbm,
    next_hbm,
    mix_ref,
    state_v,
    next_v,
    sems,
):
    seq_rows = key_unit_ref.shape[0]
    half = seq_rows // 2
    spans = [(0, half), (half, seq_rows - half)]
    loads = [
        pltpu.make_async_copy(
            state_hbm.at[pl.ds(at, size)], state_v.at[pl.ds(at, size)], sems.at[i]
        )
        for i, (at, size) in enumerate(spans)
    ]
    stores = [
        pltpu.make_async_copy(
            next_v.at[pl.ds(at, size)], next_hbm.at[pl.ds(at, size)], sems.at[2 + i]
        )
        for i, (at, size) in enumerate(spans)
    ]
    for copy in loads:
        copy.start()
    routes = columns_of(routes_ref[...].astype(jnp.float32))[:seq_rows].astype(jnp.int32)
    weights = columns_of(weights_ref[...])[:seq_rows]
    scale = weights / jnp.sum(weights, axis=1, keepdims=True) * ROUTED_SCALE
    expert_iota = lax.broadcasted_iota(jnp.int32, (seq_rows, 128), 1)
    named = jnp.zeros((seq_rows, 128), jnp.float32)
    mix = jnp.zeros((seq_rows, 128), jnp.float32)
    for route in range(routes_ref.shape[0]):
        hit = expert_iota == routes[:, route : route + 1]
        named = named + jnp.where(hit, 1.0, 0.0)
        mix = mix + jnp.where(hit, scale[:, route : route + 1], 0.0)
    chosen = earlier_rows(named)
    slots, experts = 2, 128
    chunks = mix_ref.shape[0] // 64
    spread = slots * chunks * experts
    lane = lax.broadcasted_iota(jnp.int32, (experts, spread), 1)
    place = lax.broadcasted_iota(jnp.int32, (experts, spread), 0)
    expand = jnp.where(lane // (slots * chunks) == place, 1.0, 0.0).astype(jnp.bfloat16)
    member = lax.broadcasted_iota(jnp.int32, (seq_rows, spread), 1) % (slots * chunks)
    mix_ref[...] = jnp.zeros(mix_ref.shape, mix_ref.dtype)
    for slot in range(slots):
        full = jnp.where(chosen == slot, mix, 0.0)
        high = full.astype(jnp.bfloat16)
        low = (full - high.astype(jnp.float32)).astype(jnp.bfloat16)
        for part, term in enumerate((high, low)):
            grown = jnp.dot(term, expand, preferred_element_type=jnp.float32)
            for chunk in range(chunks):
                at = (part * chunks + chunk) * 32
                kept = jnp.where(member == slot * chunks + chunk, grown, 0.0)
                mix_ref[at : at + seq_rows, :] += kept.astype(jnp.bfloat16)
    key_cols = columns_of(key_unit_ref[...])
    for part, (at, size) in enumerate(spans):
        loads[part].wait()
        for row in range(at, at + size):
            next_v[row] = (
                keep_ref[row : row + 1, :] * state_v[row]
                + key_cols[:, row : row + 1] * update_ref[row : row + 1, :]
            )
        stores[part].start()
    for copy in stores:
        copy.wait()


def rows_kernel(
    gathered_ref,
    tokens_ref,
    gain_ref,
    shared_gate_ref,
    shared_up_ref,
    shared_down_ref,
    residual_ref,
    shared_ref,
    rows_ref,
    sums_v,
    tokens_v,
    wide_v,
):
    seq_rows, width = tokens_ref.shape
    padded = tokens_v.shape[0]
    lanes = width // 128
    core = lax.axis_index("ep") % 2
    slot = lax.axis_index("tp") % 2
    group = gathered_ref.shape[0] // 2
    sent = seq_rows * lanes
    peers = rows_ref.shape[0] // (2 * lanes)
    tokens_v[...] = jnp.zeros(tokens_v.shape, jnp.float32)
    tokens_v[:seq_rows, :] = tokens_ref[...].astype(jnp.float32)
    for place in range(2):
        first = (core if place == 0 else 1 - core) * group
        summed = jnp.sum(gathered_ref[pl.ds(first, group), :sent].astype(jnp.float32), axis=0)
        sums_v[place, :sent] = summed
        sums_v[place, sent:] = jnp.zeros((padded * lanes - sent, 128), jnp.float32)
        total = jnp.concatenate(
            [sums_v[place, pl.ds(lane, padded, stride=lanes), :] for lane in range(lanes)],
            axis=1,
        )
        if place == 0:
            total = tokens_v[...] + total.astype(jnp.bfloat16).astype(jnp.float32)
        names = gathered_ref[first, sent:, :].astype(jnp.float32)
        blank = jnp.zeros((128 - names.shape[0], 128), jnp.float32)
        routes = jnp.concatenate([names, blank], axis=0).T[:padded, :6]
        picks = picked_rows(routes.astype(jnp.int32), core, slot)
        residual = total.astype(jnp.bfloat16)
        inputs = rms_rows(residual.astype(jnp.float32), gain_ref[...]).astype(jnp.bfloat16)
        if place == 0:
            residual_ref[...] = residual[:seq_rows]
            gate = jnp.dot(inputs, shared_gate_ref[...], preferred_element_type=jnp.float32)
            up = jnp.dot(inputs, shared_up_ref[...], preferred_element_type=jnp.float32)
            act = (gate / (1.0 + jnp.exp(-gate)) * up).astype(jnp.bfloat16)
            shared = jnp.dot(act, shared_down_ref[...], preferred_element_type=jnp.float32)
            shared_ref[...] = shared.astype(jnp.bfloat16)[:seq_rows]
        picked = lax.dot_general(
            picks, inputs, (((0,), (0,)), ((), ())), preferred_element_type=jnp.float32
        )
        for lane in range(lanes):
            wide_v[pl.ds(place * lanes + lane, peers, stride=2 * lanes), :] = picked[
                :, lane * 128 : (lane + 1) * 128
            ]
    rows_ref[...] = wide_v[...].astype(jnp.bfloat16)


def unpack_kernel(sent_ref, rows_ref, wide_v):
    lanes = rows_ref.shape[1] // 128
    experts = rows_ref.shape[0]
    wide_v[...] = sent_ref[...].astype(jnp.float32)
    for lane in range(lanes):
        rows_ref[:, lane * 128 : (lane + 1) * 128] = wide_v[
            pl.ds(lane, experts, stride=lanes), :
        ].astype(jnp.bfloat16)


def expert_kernel(rows_ref, own_ref, other_ref, shared_ref, blocks_ref, total_v):
    core = lax.axis_index("ep") % 2
    experts, width = rows_ref.shape
    rows = rows_ref[...]
    acts = []
    for pack_ref in (own_ref, other_ref):
        both = jnp.dot(rows, pack_ref[:width], preferred_element_type=jnp.float32)
        gate, up = both[:, :128], both[:, 128:]
        acts.append((gate / (1.0 + jnp.exp(-gate)) * up).astype(jnp.bfloat16))
    act = jnp.concatenate(acts, axis=1)
    group = blocks_ref.shape[0] // 2
    share = width // group
    peers = experts // 2
    for part in range(group):
        start = width + part * 128
        down = jnp.concatenate([own_ref[start : start + 128], other_ref[start : start + 128]], axis=0)
        total = jnp.dot(act, down, preferred_element_type=jnp.float32)
        for chunk in range(share // 128):
            total_v[chunk] = total[:, chunk * 128 : (chunk + 1) * 128]
        mine, theirs = [
            jnp.concatenate(
                [total_v[chunk, pl.ds(at, peers, stride=2), :] for chunk in range(share // 128)],
                axis=1,
            ).astype(jnp.bfloat16)
            for at in range(2)
        ]
        shared = shared_ref[:, part * share : (part + 1) * share]
        for target in range(2):
            here = core == target
            blocks_ref[target * group + part, :peers, :] = jnp.where(here, mine, theirs)
            blocks_ref[target * group + part, peers:, :] = jnp.where(
                here, shared, jnp.zeros_like(shared)
            )


def share_kernel(parts_ref, rows_ref, shared_ref, wide_v):
    share = parts_ref.shape[2]
    seq_rows = shared_ref.shape[0]
    peers = parts_ref.shape[1] - seq_rows
    group = parts_ref.shape[0] // 2
    chunks = share // 128
    stride = rows_ref.shape[0] // peers
    for source in range(2):
        for slot in range(2):
            total = parts_ref[source * group + slot, :peers, :].astype(jnp.float32)
            total += parts_ref[source * group + slot + 2, :peers, :].astype(jnp.float32)
            for chunk in range(chunks):
                at = (source * 2 + slot) * chunks + chunk
                wide_v[pl.ds(at, peers, stride=stride), :] = total[
                    :, chunk * 128 : (chunk + 1) * 128
                ]
    rows_ref[...] = wide_v[...].astype(jnp.bfloat16)
    shared = jnp.sum(parts_ref[:, peers:, :].astype(jnp.float32), axis=0)
    shared_ref[...] = shared.astype(jnp.bfloat16).astype(jnp.float32)


def final_kernel(rows_ref, mix_ref, residual_ref, shared_ref, out_ref):
    seq_rows, share = out_ref.shape
    chunks = share // 128
    found = jnp.dot(mix_ref[...], rows_ref[...], preferred_element_type=jnp.float32)
    at = pl.multiple_of(lax.axis_index("tp") * share, share)
    base = residual_ref[:, pl.ds(at, share)].astype(jnp.float32) + shared_ref[...]
    for chunk in range(chunks):
        high = found[chunk * 32 : chunk * 32 + seq_rows]
        low = found[(chunks + chunk) * 32 : (chunks + chunk) * 32 + seq_rows]
        total = base[:, chunk * 128 : (chunk + 1) * 128] + (high + low)
        out_ref[:, chunk * 128 : (chunk + 1) * 128] = total.astype(jnp.bfloat16)


def vmem():
    return pl.BlockSpec(memory_space=pltpu.VMEM)


def anywhere():
    return pl.BlockSpec(memory_space=pl.ANY)


def in_vmem(array):
    return pltpu.with_memory_space_constraint(array, pltpu.VMEM)


def per_device(
    tokens,
    delta_state,
    mixer_gain,
    query_weight,
    key_weight,
    value_weight,
    write_weight,
    decay_weight,
    decay_rate,
    decay_bias,
    head_gain,
    out_weight,
    channel_gain,
    routes,
    route_weights,
    expert_gate,
    expert_up,
    expert_down,
    shared_gate,
    shared_up,
    shared_down,
):
    seq_rows, model_width = tokens.shape
    head_dim = delta_state.shape[2]
    tp_count = lax.axis_size("tp")
    ep_count = lax.axis_size("ep")
    share_width = model_width // tp_count
    hidden = expert_gate.shape[2]
    quads = 2 * (share_width // 128)
    lanes = model_width // 128
    sent_rows = seq_rows * lanes + 8
    same_core = [[2 * p + k for p in range(ep_count // 2)] for k in range(2)]
    chips = [
        [(2 * p + k) * tp_count + t for k in range(2) for t in range(tp_count)]
        for p in range(ep_count // 2)
    ]
    f32, bf16 = jnp.float32, jnp.bfloat16
    state = delta_state.reshape(seq_rows, head_dim, head_dim)
    small = pltpu.VMEM((seq_rows, head_dim), f32)
    partials, key_unit, update, keep, packed = pl.pallas_call(
        mixer_kernel,
        out_shape=[
            jax.ShapeDtypeStruct((2 * tp_count, sent_rows, 128), bf16),
            small,
            small,
            small,
            pltpu.VMEM((3 * model_width // 2, 2 * hidden), bf16),
        ],
        in_specs=[anywhere()] * 17,
        out_specs=[anywhere()] + [vmem()] * 4,
        scratch_shapes=[
            pltpu.VMEM((seq_rows, model_width), bf16),
            pltpu.VMEM((1, model_width), f32),
            pltpu.VMEM((1, model_width), bf16),
            pltpu.VMEM((1, model_width), bf16),
            pltpu.VMEM((1, head_dim), f32),
            pltpu.SMEM((1,), f32),
            pltpu.SMEM((1,), f32),
            pltpu.VMEM(routes.T.shape, jnp.int32),
            pltpu.VMEM(routes.T.shape, f32),
            pltpu.VMEM((model_width, head_dim), bf16),
            pltpu.VMEM((model_width, head_dim), bf16),
            pltpu.VMEM((model_width, head_dim), bf16),
            pltpu.VMEM((seq_rows, head_dim, head_dim), f32),
            pltpu.VMEM((head_dim, model_width), bf16),
            pltpu.VMEM((2 * tp_count, sent_rows, 128), bf16),
            pltpu.VMEM((sent_rows, 128), f32),
            pltpu.VMEM((sent_rows, 128), f32),
            pltpu.VMEM((seq_rows, head_dim), f32),
            pltpu.VMEM((seq_rows, head_dim), f32),
            pltpu.SemaphoreType.DMA((17 + model_width // (2 * hidden),)),
        ],
    )(
        tokens,
        mixer_gain.reshape(1, model_width),
        write_weight.reshape(1, model_width),
        decay_weight.reshape(1, model_width),
        head_gain.reshape(1, head_dim),
        decay_rate,
        decay_bias,
        routes.T,
        route_weights.T,
        query_weight,
        key_weight,
        value_weight,
        state,
        out_weight,
        expert_gate[0],
        expert_up[0],
        expert_down[0],
    )
    gathered = lax.all_to_all(partials, ("ep", "tp"), 0, 0, axis_index_groups=chips, tiled=True)
    next_state, mix = pl.pallas_call(
        state_kernel,
        out_shape=[
            jax.ShapeDtypeStruct(state.shape, f32),
            pltpu.VMEM((64 * (share_width // 128), ep_count * quads), bf16),
        ],
        in_specs=[vmem()] * 5 + [anywhere()],
        out_specs=[anywhere(), vmem()],
        scratch_shapes=[
            pltpu.VMEM(state.shape, f32),
            pltpu.VMEM(state.shape, f32),
            pltpu.SemaphoreType.DMA((4,)),
        ],
    )(
        in_vmem(routes.T),
        in_vmem(route_weights.T),
        in_vmem(key_unit),
        in_vmem(update),
        in_vmem(keep),
        state,
    )
    other = lax.ppermute(packed, "tp", [(i, i ^ 1) for i in range(tp_count)])
    residual, shared_partial, outgoing = pl.pallas_call(
        rows_kernel,
        out_shape=[
            pltpu.VMEM((seq_rows, model_width), bf16),
            pltpu.VMEM((seq_rows, model_width), bf16),
            pltpu.VMEM((ep_count * lanes, 128), bf16),
        ],
        in_specs=[vmem()] * 6,
        out_specs=[vmem()] * 3,
        scratch_shapes=[
            pltpu.VMEM((2, 32 * lanes, 128), f32),
            pltpu.VMEM((32, model_width), f32),
            pltpu.VMEM((ep_count * lanes, 128), f32),
        ],
    )(
        in_vmem(gathered),
        in_vmem(tokens),
        in_vmem(channel_gain.reshape(1, model_width)),
        in_vmem(shared_gate),
        in_vmem(shared_up),
        in_vmem(shared_down),
    )
    received = lax.all_to_all(
        outgoing.reshape(ep_count // 2, 2 * lanes, 128),
        "ep",
        0,
        0,
        axis_index_groups=same_core,
        tiled=True,
    )
    rows = pl.pallas_call(
        unpack_kernel,
        out_shape=pltpu.VMEM((ep_count, model_width), bf16),
        in_specs=[vmem()],
        out_specs=vmem(),
        scratch_shapes=[pltpu.VMEM((ep_count * lanes, 128), f32)],
    )(in_vmem(received.reshape(ep_count * lanes, 128)))
    blocks = pl.pallas_call(
        expert_kernel,
        out_shape=pltpu.VMEM((2 * tp_count, ep_count // 2 + seq_rows, share_width), bf16),
        in_specs=[vmem()] * 4,
        out_specs=vmem(),
        scratch_shapes=[
            pltpu.VMEM((share_width // 128, ep_count, 128), f32),
        ],
    )(
        in_vmem(rows),
        in_vmem(packed),
        in_vmem(other),
        in_vmem(shared_partial),
    )
    parts = lax.all_to_all(
        blocks, ("ep", "tp"), 0, 0, axis_index_groups=chips, tiled=True
    )
    expert_share, shared_out = pl.pallas_call(
        share_kernel,
        out_shape=[
            pltpu.VMEM((ep_count * quads, 128), bf16),
            pltpu.VMEM((seq_rows, share_width), f32),
        ],
        in_specs=[vmem()],
        out_specs=[vmem()] * 2,
        scratch_shapes=[pltpu.VMEM((ep_count * quads, 128), f32)],
    )(in_vmem(parts))
    returned = lax.all_to_all(
        expert_share.reshape(ep_count // 2, 2 * quads, 128),
        "ep",
        0,
        0,
        axis_index_groups=same_core,
        tiled=True,
    )
    layer_out = pl.pallas_call(
        final_kernel,
        out_shape=jax.ShapeDtypeStruct((seq_rows, share_width), bf16),
        in_specs=[vmem()] * 4,
        out_specs=vmem(),
    )(
        in_vmem(returned.reshape(ep_count * quads, 128)),
        in_vmem(mix),
        in_vmem(residual),
        in_vmem(shared_out),
    )
    return (layer_out, next_state.reshape(delta_state.shape))


def solution(mesh):
    return jax.shard_map(
        per_device,
        mesh=mesh,
        in_specs=(
            P("ep", None),
            P("ep", "tp", None, None),
            P(),
            P(None, "tp"),
            P(None, "tp"),
            P(None, "tp"),
            P(None, "tp"),
            P(None, "tp"),
            P("tp"),
            P("tp"),
            P(),
            P("tp", None),
            P(),
            P("ep", None),
            P("ep", None),
            P("ep", None, "tp"),
            P("ep", None, "tp"),
            P("ep", "tp", None),
            P(None, "tp"),
            P(None, "tp"),
            P("tp", None),
        ),
        out_specs=(P("ep", "tp"), P("ep", "tp", None, None)),
        check_vma=False,
    )
```
